512 devices in a mesh: fs: 128 (over z, y, core), tp: 4 (over x).
Axes of the slice: x: 4, y: 8, z: 8, core: 2. Of those that a mesh axis runs over, the one named last changes fastest.
Arguments:
- prompt_tokens: bfloat16 [768, 4096], P('tp'), may hold values from -6 to 6
- norm_gain: float32 [4096], P('fs'), may hold values from 0.1 to 1.9
- gate_trained: float32 [4096, 11264], P('fs', 'tp'), may hold values from -0.09375 to 0.09375
- up_trained: float32 [4096, 11264], P('fs', 'tp'), may hold values from -0.09375 to 0.09375
- down_trained: float32 [11264, 4096], P('fs', 'tp'), may hold values from -0.21875 to 0.21875
Outputs:
- gate_serving: bfloat16 [4096, 11264], P(None, 'fs')
- up_serving: bfloat16 [4096, 11264], P(None, 'fs')
- down_serving: bfloat16 [11264, 4096], P('fs')
- mixed: bfloat16 [768, 4096], P('tp', 'fs')
The draws below stay inside these ranges and needn't reach their ends.
All inputs are finite; a program needn't handle non-finite values.
Results may differ from the reference program's by a relative error of at most 0.0082.
Values may be sent and summed in bfloat16 or wider, within the bound.
A program may use at most 64 MiB of HBM per device.

```python
import jax
import jax.numpy as jnp
from jax import lax

D = 4096
FF = 11264
TOKENS = 768


def with_spikes(entries, key, source, target, shards_of, factor):
    def block_of(dim):
        return (jnp.arange(entries.shape[dim]) // (entries.shape[dim] // shards_of)).reshape((-1,) + (1,) * (entries.ndim - 1 - dim))

    near = jax.random.permutation(key, shards_of)[block_of(target)]
    second = (block_of(target) + shards_of // 2) % shards_of
    return jnp.where((block_of(source) == near) | (block_of(source) == second), factor * entries, entries)


def levels(stream_key, extent, shards, low, high):
    def one(axis_at, blocks):
        heights = jax.random.uniform(jax.random.fold_in(jax.random.fold_in(stream_key, 6), axis_at), (blocks,), jnp.float32, low / len(shards), high / len(shards))
        return jnp.repeat(jnp.exp(heights), extent[axis_at] // blocks).reshape((-1,) + (1,) * (len(extent) - axis_at - 1))

    level = one(*shards[0])
    for cut in shards[1:]:
        level = level * one(*cut)
    return level


def scatter_about(stream_key, dims, scale, reach, cuts=(), dtype=jnp.bfloat16):
    entries = scale * jax.random.normal(stream_key, dims, jnp.float32)
    if cuts:
        entries = entries * levels(stream_key, dims, cuts, -0.22, 0.18)
    return jnp.clip(entries, -reach, reach).astype(dtype)


def heavy_noise(stream_key, dims, scale, bound, shards, heavy, dtype=jnp.bfloat16):
    values = scale * jax.random.normal(stream_key, dims, jnp.float32)
    if shards:
        values = values * levels(stream_key, dims, shards, -0.22, 0.18)
    return jnp.clip(with_spikes(values, jax.random.fold_in(stream_key, 3), *heavy), -bound, bound).astype(dtype)


def setup_inputs(seed: int = 0) -> dict:
    splits = jax.random.split(jax.random.key(seed), 6)
    return {
        "prompt_tokens": scatter_about(splits[0], (TOKENS, D), 1.0, 6.0, ((0, 4),)),
        "norm_gain": jnp.clip(1.0 + 0.18 * jax.random.normal(splits[1], (D,), jnp.float32), 0.1, 1.9),
        "gate_trained": scatter_about(splits[2], (D, FF), D ** -0.5, 0.09375, ((0, 128), (1, 4)), jnp.float32),
        "up_trained": scatter_about(splits[3], (D, FF), D ** -0.5, 0.09375, ((0, 128), (1, 4)), jnp.float32),
        "down_trained": heavy_noise(splits[4], (FF, D), FF ** -0.5, 0.21875, ((0, 128), (1, 4)), (0, 1, 128, 5.5), jnp.float32),
    }


def reference(prompt_tokens, norm_gain, gate_trained, up_trained, down_trained):
    gate_serving = (gate_trained * norm_gain[:, None]).astype(jnp.bfloat16)
    up_serving = (up_trained * norm_gain[:, None]).astype(jnp.bfloat16)
    down_serving = down_trained.astype(jnp.bfloat16)
    tokens = prompt_tokens.astype(jnp.float32)
    scale = jax.lax.rsqrt(lax.optimization_barrier(jnp.mean(tokens * tokens, axis=-1, keepdims=True)) + 1e-06)
    normed = (tokens * scale).astype(jnp.bfloat16)
    gate = jnp.dot(normed, gate_serving, preferred_element_type=jnp.float32)
    up = jnp.dot(normed, up_serving, preferred_element_type=jnp.float32)
    hidden = (jax.nn.silu(gate) * up).astype(jnp.bfloat16)
    mixed = jnp.dot(hidden, down_serving, preferred_element_type=jnp.float32).astype(jnp.bfloat16)
    return (gate_serving, up_serving, down_serving, mixed)
```

```python
import jax
import jax.numpy as jnp
from jax import lax
from jax.experimental import pallas as pl
from jax.experimental.pallas import tpu as pltpu
from jax.sharding import Mesh
from jax.sharding import PartitionSpec as P

MESH = pl.DeviceIdType.MESH
AXES = ("fz", "fy", "fc", "tp")
BF16 = jnp.bfloat16
F32 = jnp.float32
FAR_FIRST = (4, 3, 5, 2, 6, 1, 7)


def remote(src, dst, send, recv, device):
    return pltpu.make_async_remote_copy(
        src_ref=src, dst_ref=dst, send_sem=send, recv_sem=recv, device_id=device, device_id_type=MESH
    )


def kernel(
    tokens_hbm, gain_ref, gate_hbm, up_hbm, down_hbm,
    gate_out, up_out, down_out, mixed_out,
    tok, gate_in, up_in, down_in, packed, r1, r2, w, normed, db, parts, got, pieces, got2, last, mix, gate_v, up_v,
    in_sem, out_sem, xs, xr, as_, ar, bs, br, ds, dr, gs, gr, cs, cr, es, er, ps, pr, qs, qr, fs, fr,
):
    z, y, c, x = (lax.axis_index(a) for a in AXES)
    right, left, opposite = lax.rem(x + 1, 4), lax.rem(x + 3, 4), lax.rem(x + 2, 4)
    partner = (z, y, 1 - c, x)

    def x_peer(p):
        return (z, y, c, p)

    first = jnp.where(c == 0, y, z)
    second = jnp.where(c == 0, z, y)

    def first_peer(p):
        return (jnp.where(c == 0, z, p), jnp.where(c == 0, p, y), c, x)

    def second_peer(p):
        return (jnp.where(c == 0, p, z), jnp.where(c == 0, y, p), c, x)

    barrier = pltpu.get_barrier_semaphore()
    peers = [x_peer(lax.rem(x + k, 4)) for k in (1, 2, 3)]
    peers += [first_peer(lax.rem(first + k, 8)) for k in range(1, 8)]
    peers += [second_peer(lax.rem(second + k, 8)) for k in range(1, 8)]
    peers += [partner]
    for peer in peers:
        pl.semaphore_signal(barrier, inc=1, device_id=peer, device_id_type=MESH)

    row = pl.multiple_of(96 * c, 32)
    loads = [
        pltpu.make_async_copy(gate_hbm, gate_in, in_sem.at[0]),
        pltpu.make_async_copy(up_hbm, up_in, in_sem.at[1]),
        pltpu.make_async_copy(down_hbm, down_in, in_sem.at[2]),
        pltpu.make_async_copy(tokens_hbm.at[pl.ds(row, 96)], tok, in_sem.at[3]),
    ]
    for load in loads:
        load.start()

    lanes = lax.broadcasted_iota(jnp.int32, (32, 32), 1)
    rows = lax.broadcasted_iota(jnp.int32, (32, 32), 0)
    spread = jnp.broadcast_to(gain_ref[...], (32, 32))
    gain = jnp.sum(jnp.where(lanes == rows, spread, 0.0), axis=1, keepdims=True)
    loads[0].wait()
    loads[1].wait()
    for s in range(4):
        scale = gain[8 * s : 8 * s + 8]
        g = gate_in[8 * s : 8 * s + 8, :] * scale
        u = up_in[8 * s : 8 * s + 8, :] * scale
        for j in range(16):
            cut = slice(176 * j, 176 * j + 176)
            unit = jnp.concatenate([g[:, cut], u[:, cut], jnp.zeros((8, 32), F32)], axis=1)
            packed[s, j // 8, j % 8] = unit.astype(BF16)

    pl.semaphore_wait(barrier, 18)

    x_sends = []
    for k in (2, 1, 3):
        p = lax.rem(x + k, 4)
        send = remote(packed.at[p], r1.at[pl.ds(2 * x, 2)], xs.at[k], xr.at[k], x_peer(p))
        send.start()
        x_sends.append(send)
    r1[pl.ds(2 * x, 2)] = packed[x]

    loads[2].wait()
    for i in range(11):
        db[c, x, i] = down_in[8 * i : 8 * i + 8, :].astype(BF16)

    def down_half(t, h):
        return db.at[c, t, :, :, pl.ds(512 * h, 512)]

    def down_copy(t, h, k, p):
        return remote(down_half(t, h), down_half(t, h), ds.at[k], dr.at[k], x_peer(p))

    d_sends = [
        down_copy(x, 0, 0, right), down_copy(x, 1, 1, left), down_copy(x, 1, 2, right), down_copy(x, 0, 3, left)
    ]
    for send in d_sends:
        send.start()

    for send in x_sends:
        send.wait_recv()

    a_sends = []
    for k in FAR_FIRST:
        p = lax.rem(first + k, 8)

        @pl.when(c == 0)
        def _():
            remote(r1.at[:, p], r2.at[first], as_.at[k], ar.at[k], first_peer(p)).start()

        @pl.when(c == 1)
        def _():
            remote(r1.at[p], r2.at[first], as_.at[k], ar.at[k], first_peer(p)).start()

        a_sends.append(remote(r1.at[p], r2.at[first], as_.at[k], ar.at[k], first_peer(p)))

    @pl.when(c == 0)
    def _():
        r2[first] = r1[:, first]

    @pl.when(c == 1)
    def _():
        r2[first] = r1[first]

    loads[3].wait()

    def norm_rows(i, carry):
        part = tok[pl.ds(pl.multiple_of(16 * i, 16), 16), :].astype(F32)
        mean = jnp.mean(part * part, axis=-1, keepdims=True)
        normed[pl.ds(pl.multiple_of(16 * i, 16), 16), :] = (part * lax.rsqrt(mean + 1e-06)).astype(BF16)
        return carry

    lax.fori_loop(0, 6, norm_rows, 0)

    for send in a_sends:
        send.wait_recv()

    b_sends = []
    for k in FAR_FIRST:
        p = lax.rem(second + k, 8)

        @pl.when(c == 0)
        def _():
            remote(r2.at[:, p], w.at[second, :, c, x], bs.at[k], br.at[k], second_peer(p)).start()

        @pl.when(c == 1)
        def _():
            remote(r2.at[:, p], w.at[:, second, c, x], bs.at[k], br.at[k], second_peer(p)).start()

        b_sends.append(remote(r2.at[:, p], w.at[second, :, c, x], bs.at[k], br.at[k], second_peer(p)))

    @pl.when(c == 0)
    def _():
        w[second, :, c, x] = r2[:, second]

    @pl.when(c == 1)
    def _():
        w[:, second, c, x] = r2[:, second]

    d_sends[0].wait_recv()
    forward = down_copy(left, 0, 4, right)
    forward.start()
    d_sends.append(forward)
    d_sends[1].wait_recv()
    forward = down_copy(right, 1, 5, left)
    forward.start()
    d_sends.append(forward)

    for send in b_sends:
        send.wait_recv()

    def block(core, s, h, g):
        return w.at[pl.ds(4 * h, 4), pl.ds(4 * g, 4), core, s]

    def gather_copy(s, h, g, k, p):
        return remote(block(c, s, h, g), block(c, s, h, g), gs.at[h, k], gr.at[h, k], x_peer(p))

    def core_copy(s, h, g, k):
        return remote(block(c, s, h, g), block(c, s, h, g), cs.at[h, k], cr.at[h, k], partner)

    g_sends = []
    c_sends = []
    acc = jnp.zeros((96, 384), F32)
    for h in range(2):
        ways = [
            gather_copy(x, h, 0, 0, right), gather_copy(x, h, 1, 1, left),
            gather_copy(x, h, 1, 2, right), gather_copy(x, h, 0, 3, left),
        ]
        for send in ways:
            send.start()
        swaps = []

        def swap(s, g, k):
            send = core_copy(s, h, g, k)
            send.start()
            swaps.append(send)

        swap(x, 0, 0)
        swap(x, 1, 1)
        ways[0].wait_recv()
        forward = gather_copy(left, h, 0, 4, right)
        forward.start()
        ways.append(forward)
        swap(left, 0, 2)
        ways[1].wait_recv()
        forward = gather_copy(right, h, 1, 5, left)
        forward.start()
        ways.append(forward)
        swap(right, 1, 3)
        ways[2].wait_recv()
        swap(left, 1, 4)
        ways[3].wait_recv()
        swap(right, 0, 5)
        g_sends.append(ways)
        c_sends.append(swaps)
        if h == 0:
            for send in d_sends[2:]:
                send.wait_recv()
            whole = remote(db.at[c], db.at[c], es, er, partner)
            whole.start()
    for h in range(2):
        for k, g in ((4, 0), (5, 1)):
            g_sends[h][k].wait_recv()
            send = core_copy(opposite, h, g, 6 + g)
            send.start()
            c_sends[h].append(send)
        for send in c_sends[h]:
            send.wait_recv()
        acc += jnp.dot(
            normed[:, 2048 * h : 2048 * h + 2048],
            w[4 * h : 4 * h + 4].reshape(2048, 384),
            preferred_element_type=F32,
        )
    gate = acc[:, :176]
    up = acc[:, 176:352]
    hidden = (gate * (1.0 / (1.0 + jnp.exp(-gate))) * up).astype(BF16)
    whole.wait_recv()

    def piece_send(p, k):
        return remote(parts.at[p], got.at[first], ps.at[k], pr.at[k], first_peer(p))

    @pl.when(c == 0)
    def _():
        for p in range(8):
            cols = [
                db[:, q // 2, :, :, 512 * (q % 2) + 64 * p : 512 * (q % 2) + 64 * p + 64].reshape(176, 64)
                for q in range(8)
            ]
            parts[p] = jnp.dot(hidden, jnp.concatenate(cols, axis=1), preferred_element_type=F32).astype(BF16)

    @pl.when(c == 1)
    def _():
        for p in range(8):
            cols = db[:, p // 2, :, :, 512 * (p % 2) : 512 * (p % 2) + 512].reshape(176, 512)
            parts[p] = jnp.dot(hidden, cols, preferred_element_type=F32).astype(BF16)

    p_sends = []
    for k in FAR_FIRST:
        send = piece_send(lax.rem(first + k, 8), k)
        send.start()
        p_sends.append(send)

    for core in range(2):
        @pl.when(c == core)
        def _():
            def unpack(i, carry):
                rows = w[i]
                gate_v[i] = rows[..., 88 * core : 88 * core + 88]
                up_v[i] = rows[..., 176 + 88 * core : 264 + 88 * core]
                return carry

            lax.fori_loop(0, 8, unpack, 0)

    outs = [
        pltpu.make_async_copy(gate_v, gate_out, out_sem.at[0]),
        pltpu.make_async_copy(up_v, up_out, out_sem.at[1]),
    ]
    for t in range(4):
        outs.append(pltpu.make_async_copy(db.at[c, t], down_out.at[:, :, pl.ds(1024 * t, 1024)], out_sem.at[2 + t]))
    for out in outs:
        out.start()

    for send in p_sends:
        send.wait_recv()
    total = parts[first].astype(F32)
    for k in FAR_FIRST:
        total += got[lax.rem(first + k, 8)].astype(F32)
    for q in range(8):
        pieces[q] = total[:, 64 * q : 64 * q + 64].astype(BF16)
    q_sends = []
    for k in FAR_FIRST:
        p = lax.rem(second + k, 8)
        send = remote(pieces.at[p], got2.at[second], qs.at[k], qr.at[k], second_peer(p))
        send.start()
        q_sends.append(send)
    for send in q_sends:
        send.wait_recv()
    total = pieces[second].astype(F32)
    for k in FAR_FIRST:
        total += got2[lax.rem(second + k, 8)].astype(F32)

    @pl.when(c == 0)
    def _():
        mix[c] = total[:, :32].astype(BF16)
        last[...] = total[:, 32:].astype(BF16)

    @pl.when(c == 1)
    def _():
        mix[c] = total[:, 32:].astype(BF16)
        last[...] = total[:, :32].astype(BF16)

    swap_last = remote(last, mix.at[c], fs, fr, partner)
    swap_last.start()
    swap_last.wait_recv()
    out = pltpu.make_async_copy(mix, mixed_out, out_sem.at[6])
    out.start()
    for send in x_sends + d_sends + a_sends + b_sends + p_sends + q_sends:
        send.wait_send()
    for ways in g_sends + c_sends:
        for send in ways:
            send.wait_send()
    whole.wait_send()
    swap_last.wait_send()
    for out_copy in outs:
        out_copy.wait()
    out.wait()


def on_device(prompt_tokens, norm_gain, gate_trained, up_trained, down_trained):
    dma = pltpu.SemaphoreType.DMA
    hbm = pl.BlockSpec(memory_space=pl.ANY)
    vmem = pltpu.VMEM
    gate, up, down, mixed = pl.pallas_call(
        kernel,
        out_shape=(
            jax.ShapeDtypeStruct((8, 8, 2, 4, 8, 88), BF16),
            jax.ShapeDtypeStruct((8, 8, 2, 4, 8, 88), BF16),
            jax.ShapeDtypeStruct((11, 8, 4096), BF16),
            jax.ShapeDtypeStruct((2, 96, 32), BF16),
        ),
        in_specs=[hbm, pl.BlockSpec(memory_space=pltpu.VMEM), hbm, hbm, hbm],
        out_specs=(hbm, hbm, hbm, hbm),
        scratch_shapes=[
            vmem((96, 4096), BF16),
            vmem((32, 2816), F32),
            vmem((32, 2816), F32),
            vmem((88, 1024), F32),
            vmem((4, 2, 8, 8, 384), BF16),
            vmem((8, 8, 8, 384), BF16),
            vmem((8, 8, 8, 384), BF16),
            vmem((8, 8, 2, 4, 8, 384), BF16),
            vmem((96, 4096), BF16),
            vmem((2, 4, 11, 8, 1024), BF16),
            vmem((8, 96, 512), BF16),
            vmem((8, 96, 512), BF16),
            vmem((8, 96, 64), BF16),
            vmem((8, 96, 64), BF16),
            vmem((96, 32), BF16),
            vmem((2, 96, 32), BF16),
            vmem((8, 8, 2, 4, 8, 88), BF16),
            vmem((8, 8, 2, 4, 8, 88), BF16),
            dma((4,)), dma((7,)),
            dma((4,)), dma((4,)),
            dma((8,)), dma((8,)),
            dma((8,)), dma((8,)),
            dma((6,)), dma((6,)),
            dma((2, 6)), dma((2, 6)),
            dma((2, 8)), dma((2, 8)),
            dma, dma,
            dma((8,)), dma((8,)),
            dma((8,)), dma((8,)),
            dma, dma,
        ],
        compiler_params=pltpu.CompilerParams(
            collective_id=0, has_side_effects=True, vmem_limit_bytes=48 * 1024 * 1024
        ),
    )(prompt_tokens, norm_gain.reshape(1, 32), gate_trained, up_trained, down_trained)
    return gate.reshape(4096, 88), up.reshape(4096, 88), down.reshape(88, 4096), mixed.reshape(192, 32)


def solution(mesh):
    finer = Mesh(mesh.devices.reshape(8, 8, 2, mesh.shape["tp"]), AXES)
    rows = AXES[:3]
    return jax.shard_map(
        on_device,
        mesh=finer,
        in_specs=(P("tp", None), P(rows), P(rows, "tp"), P(rows, "tp"), P(rows, "tp")),
        out_specs=(P(None, rows), P(None, rows), P(rows, None), P("tp", rows)),
        check_vma=False,
    )
```

```python
import jax
import jax.numpy as jnp
from jax import lax
from jax.experimental import pallas as pl
from jax.experimental.pallas import tpu as pltpu
from jax.sharding import Mesh
from jax.sharding import PartitionSpec as P

MESH = pl.DeviceIdType.MESH
AXES = ("fz", "fy", "fc", "tp")
BF16 = jnp.bfloat16
F32 = jnp.float32
LIMIT = 40 * 1024 * 1024
FAR_FIRST = (4, 3, 5, 2, 6, 1, 7)


def remote(src, dst, send, recv, device):
    return pltpu.make_async_remote_copy(
        src_ref=src, dst_ref=dst, send_sem=send, recv_sem=recv, device_id=device, device_id_type=MESH
    )


class Flights:
    def __init__(self):
        self.all = []
        self.landed = set()

    def note(self, copy):
        self.all.append(copy)
        return copy

    def go(self, copy):
        copy.start()
        return self.note(copy)

    def land(self, copy):
        copy.wait_recv()
        self.landed.add(id(copy))

    def finish(self):
        for copy in self.all:
            if id(copy) not in self.landed:
                copy.wait_recv()
        for copy in self.all:
            copy.wait_send()


def kernel(
    tokens_hbm, gain_hbm, gate_hbm, up_hbm, down_hbm,
    gate_out, up_out, down_out, mixed_out,
    tok, gain_in, gate_in, up_in, down_in, packed, r1, r2, w, normed, db, parts, got, pieces, got2, last, mix,
    in_sem, xs, xr, as_, ar, bs, br, ds, dr, gs, gr, cs, cr, es, er, ps, pr, qs, qr, fs, fr,
):
    z, y, c, x = (lax.axis_index(a) for a in AXES)
    right, left, opposite = lax.rem(x + 1, 4), lax.rem(x + 3, 4), lax.rem(x + 2, 4)
    partner = (z, y, 1 - c, x)
    flights = Flights()
    go, land = flights.go, flights.land

    def x_peer(p):
        return (z, y, c, p)

    first = jnp.where(c == 0, y, z)
    second = jnp.where(c == 0, z, y)

    def first_peer(p):
        return (jnp.where(c == 0, z, p), jnp.where(c == 0, p, y), c, x)

    def second_peer(p):
        return (jnp.where(c == 0, p, z), jnp.where(c == 0, y, p), c, x)

    barrier = pltpu.get_barrier_semaphore()
    peers = [x_peer(lax.rem(x + k, 4)) for k in (1, 2, 3)]
    peers += [first_peer(lax.rem(first + k, 8)) for k in range(1, 8)]
    peers += [second_peer(lax.rem(second + k, 8)) for k in range(1, 8)]
    peers += [partner]
    row = pl.multiple_of(96 * c, 32)
    loads = [
        pltpu.make_async_copy(gate_hbm, gate_in, in_sem.at[0]),
        pltpu.make_async_copy(up_hbm, up_in, in_sem.at[1]),
        pltpu.make_async_copy(down_hbm, down_in, in_sem.at[2]),
        pltpu.make_async_copy(tokens_hbm.at[pl.ds(row, 96)], tok, in_sem.at[3]),
        pltpu.make_async_copy(gain_hbm, gain_in, in_sem.at[4]),
    ]
    for load in loads:
        load.start()
    for peer in peers:
        pl.semaphore_signal(barrier, inc=1, device_id=peer, device_id_type=MESH)

    lanes = lax.broadcasted_iota(jnp.int32, (32, 32), 1)
    rows = lax.broadcasted_iota(jnp.int32, (32, 32), 0)
    loads[4].wait()
    spread = jnp.broadcast_to(gain_in[...], (32, 32))
    gain = jnp.sum(jnp.where(lanes == rows, spread, 0.0), axis=1, keepdims=True)
    loads[0].wait()
    loads[1].wait()
    for s in range(4):
        scale = gain[8 * s : 8 * s + 8]
        g = gate_in[8 * s : 8 * s + 8, :] * scale
        u = up_in[8 * s : 8 * s + 8, :] * scale
        for j in range(16):
            cut = slice(176 * j, 176 * j + 176)
            unit = jnp.concatenate([g[:, cut], u[:, cut], jnp.zeros((8, 32), F32)], axis=1).astype(BF16)
            for n in range(3):
                packed[n, s, j // 8, j % 8] = unit[:, 128 * n : 128 * n + 128]

    pl.semaphore_wait(barrier, 18)
    x_sends = []
    for n in range(3):
        x_sends.append([])
        for k in (2, 1, 3):
            p = lax.rem(x + k, 4)
            x_sends[n].append(
                go(remote(packed.at[n, p], r1.at[n, pl.ds(2 * x, 2)], xs.at[n, k], xr.at[n, k], x_peer(p)))
            )

    loads[2].wait()
    for i in range(11):
        db[c, x, i] = down_in[8 * i : 8 * i + 8, :].astype(BF16)

    def down_copy(t, h, k, p):
        half = db.at[c, t, :, :, pl.ds(512 * h, 512)]
        return remote(half, half, ds.at[k], dr.at[k], x_peer(p))

    d_ways = [
        go(down_copy(x, 0, 0, right)), go(down_copy(x, 1, 1, left)),
        go(down_copy(x, 1, 2, right)), go(down_copy(x, 0, 3, left)),
    ]

    for n in range(3):
        r1[n, pl.ds(2 * x, 2)] = packed[n, x]

    a_sends = []
    for n in range(3):
        for send in x_sends[n]:
            land(send)
        a_sends.append([])
        for k in FAR_FIRST:
            p = lax.rem(first + k, 8)
            sems = as_.at[n, k], ar.at[n, k]

            @pl.when(c == 0)
            def _():
                remote(r1.at[n, :, p], r2.at[n, first], *sems, first_peer(p)).start()

            @pl.when(c == 1)
            def _():
                remote(r1.at[n, p], r2.at[n, first], *sems, first_peer(p)).start()

            a_sends[n].append(flights.note(remote(r1.at[n, p], r2.at[n, first], *sems, first_peer(p))))

        @pl.when(c == 0)
        def _():
            r2[n, first] = r1[n, :, first]

        @pl.when(c == 1)
        def _():
            r2[n, first] = r1[n, first]

    loads[3].wait()

    def norm_rows(i, carry):
        part = tok[pl.ds(pl.multiple_of(16 * i, 16), 16), :].astype(F32)
        mean = jnp.mean(part * part, axis=-1, keepdims=True)
        normed[pl.ds(pl.multiple_of(16 * i, 16), 16), :] = (part * lax.rsqrt(mean + 1e-06)).astype(BF16)
        return carry

    lax.fori_loop(0, 6, norm_rows, 0)

    b_sends = []
    for n in range(3):
        for send in a_sends[n]:
            land(send)
        b_sends.append([])
        for k in FAR_FIRST:
            p = lax.rem(second + k, 8)
            sems = bs.at[n, k], br.at[n, k]

            @pl.when(c == 0)
            def _():
                remote(r2.at[n, :, p], w.at[n, second, :, c, x], *sems, second_peer(p)).start()

            @pl.when(c == 1)
            def _():
                remote(r2.at[n, :, p], w.at[n, :, second, c, x], *sems, second_peer(p)).start()

            b_sends[n].append(
                flights.note(remote(r2.at[n, :, p], w.at[n, second, :, c, x], *sems, second_peer(p)))
            )

        @pl.when(c == 0)
        def _():
            w[n, second, :, c, x] = r2[n, :, second]

        @pl.when(c == 1)
        def _():
            w[n, :, second, c, x] = r2[n, :, second]

        if n == 0:
            land(d_ways[0])
            d_ways.append(go(down_copy(left, 0, 4, right)))
            land(d_ways[1])
            d_ways.append(go(down_copy(right, 1, 5, left)))

    def gather_copy(s, n, h, k, p):
        half = w.at[n, :, pl.ds(4 * h, 4), c, s]
        return remote(half, half, gs.at[n, k], gr.at[n, k], x_peer(p))

    def core_copy(s, n, k):
        return remote(w.at[n, :, :, c, s], w.at[n, :, :, c, s], cs.at[n, k], cr.at[n, k], partner)

    ways = []
    swaps = []
    for n in range(3):
        for send in b_sends[n]:
            land(send)
        ways.append([
            go(gather_copy(x, n, 0, 0, right)), go(gather_copy(x, n, 1, 1, left)),
            go(gather_copy(x, n, 1, 2, right)), go(gather_copy(x, n, 0, 3, left)),
        ])
        swaps.append([go(core_copy(x, n, 0))])
    for send in d_ways[2:]:
        land(send)
    whole = go(remote(db.at[c], db.at[c], es, er, partner))
    for n in range(3):
        land(ways[n][0])
        ways[n].append(go(gather_copy(left, n, 0, 4, right)))
        land(ways[n][1])
        ways[n].append(go(gather_copy(right, n, 1, 5, left)))
        land(ways[n][2])
        swaps[n].append(go(core_copy(left, n, 1)))
        land(ways[n][3])
        swaps[n].append(go(core_copy(right, n, 2)))
    acc = []
    for n in range(3):
        land(ways[n][4])
        land(ways[n][5])
        swaps[n].append(go(core_copy(opposite, n, 3)))
        for send in swaps[n]:
            land(send)
        acc.append(jnp.dot(normed[...], w[n].reshape(4096, 128), preferred_element_type=F32))
    gate = jnp.concatenate([acc[0], acc[1][:, :48]], axis=1)
    up = jnp.concatenate([acc[1][:, 48:], acc[2][:, :96]], axis=1)
    hidden = (gate * (1.0 / (1.0 + jnp.exp(-gate))) * up).astype(BF16)
    land(whole)

    @pl.when(c == 0)
    def _():
        for p in range(8):
            cols = [
                db[:, q // 2, :, :, 512 * (q % 2) + 64 * p : 512 * (q % 2) + 64 * p + 64].reshape(176, 64)
                for q in range(8)
            ]
            parts[p] = jnp.dot(hidden, jnp.concatenate(cols, axis=1), preferred_element_type=F32).astype(BF16)

    @pl.when(c == 1)
    def _():
        for p in range(8):
            cols = db[:, p // 2, :, :, 512 * (p % 2) : 512 * (p % 2) + 512].reshape(176, 512)
            parts[p] = jnp.dot(hidden, cols, preferred_element_type=F32).astype(BF16)

    p_sends = []
    for k in FAR_FIRST:
        p = lax.rem(first + k, 8)
        p_sends.append(go(remote(parts.at[p], got.at[first], ps.at[k], pr.at[k], first_peer(p))))

    for core in range(2):
        @pl.when(c == core)
        def _():
            def unpack(i, carry):
                at = pl.ds(pl.multiple_of(512 * i, 512), 512)
                tiles = [w[n, i].reshape(512, 128).T for n in range(3)]
                for out, start in ((gate_out, 88 * core), (up_out, 176 + 88 * core)):
                    for r in range(11):
                        n, k = divmod(start + 8 * r, 128)
                        out[r, :, at] = tiles[n][k : k + 8]
                return carry

            lax.fori_loop(0, 8, unpack, 0)
    for t in range(4):
        down_out[:, :, 1024 * t : 1024 * t + 1024] = db[c, t]

    for send in p_sends:
        land(send)
    total = parts[first].astype(F32)
    for k in FAR_FIRST:
        total += got[lax.rem(first + k, 8)].astype(F32)
    for q in range(8):
        both = jnp.concatenate([total[:48, 64 * q : 64 * q + 64], total[48:, 64 * q : 64 * q + 64]], axis=1)
        pieces[q] = both.astype(BF16)
    q_sends = []
    for k in FAR_FIRST:
        p = lax.rem(second + k, 8)
        q_sends.append(go(remote(pieces.at[p], got2.at[second], qs.at[k], qr.at[k], second_peer(p))))
    for send in q_sends:
        land(send)
    total = pieces[second].astype(F32)
    for k in FAR_FIRST:
        total += got2[lax.rem(second + k, 8)].astype(F32)
    total = jnp.concatenate([total[:, :64], total[:, 64:]], axis=0)

    @pl.when(c == 0)
    def _():
        mix[c] = total[:, :32].astype(BF16)
        last[...] = total[:, 32:].astype(BF16)

    @pl.when(c == 1)
    def _():
        mix[c] = total[:, 32:].astype(BF16)
        last[...] = total[:, :32].astype(BF16)

    land(go(remote(last, mix.at[c], fs, fr, partner)))
    mixed_out[...] = jnp.concatenate([mix[0], mix[1]], axis=0).astype(F32).T.astype(BF16)
    flights.finish()


def write_out(*refs):
    sem = refs[-1]
    copies = [pltpu.make_async_copy(refs[k], refs[k + 4], sem.at[k]) for k in range(4)]
    for copy in copies:
        copy.start()
    for copy in copies:
        copy.wait()


def on_device(prompt_tokens, norm_gain, gate_trained, up_trained, down_trained):
    dma = pltpu.SemaphoreType.DMA
    hbm = pl.BlockSpec(memory_space=pltpu.HBM)
    in_vmem = pl.BlockSpec(memory_space=pltpu.VMEM)
    vmem = pltpu.VMEM
    shapes = (
        jax.ShapeDtypeStruct((11, 8, 4096), BF16),
        jax.ShapeDtypeStruct((11, 8, 4096), BF16),
        jax.ShapeDtypeStruct((11, 8, 4096), BF16),
        jax.ShapeDtypeStruct((32, 192), BF16),
    )
    results = pl.pallas_call(
        kernel,
        out_shape=[pltpu.VMEM(a.shape, a.dtype) for a in shapes],
        in_specs=[hbm] * 5,
        out_specs=(in_vmem,) * 4,
        scratch_shapes=[
            vmem((96, 4096), BF16),
            vmem((1, 32), F32),
            vmem((32, 2816), F32),
            vmem((32, 2816), F32),
            vmem((88, 1024), F32),
            vmem((3, 4, 2, 8, 8, 128), BF16),
            vmem((3, 8, 8, 8, 128), BF16),
            vmem((3, 8, 8, 8, 128), BF16),
            vmem((3, 8, 8, 2, 4, 8, 128), BF16),
            vmem((96, 4096), BF16),
            vmem((2, 4, 11, 8, 1024), BF16),
            vmem((8, 96, 512), BF16),
            vmem((8, 96, 512), BF16),
            vmem((8, 48, 128), BF16),
            vmem((8, 48, 128), BF16),
            vmem((96, 32), BF16),
            vmem((2, 96, 32), BF16),
            dma((5,)),
            dma((3, 4)), dma((3, 4)),
            dma((3, 8)), dma((3, 8)),
            dma((3, 8)), dma((3, 8)),
            dma((6,)), dma((6,)),
            dma((3, 6)), dma((3, 6)),
            dma((3, 4)), dma((3, 4)),
            dma, dma,
            dma((8,)), dma((8,)),
            dma((8,)), dma((8,)),
            dma, dma,
        ],
        compiler_params=pltpu.CompilerParams(
            collective_id=0, has_side_effects=True, vmem_limit_bytes=LIMIT
        ),
    )(
        pltpu.with_memory_space_constraint(prompt_tokens, pltpu.HBM),
        pltpu.with_memory_space_constraint(norm_gain.reshape(1, 32), pltpu.HBM),
        pltpu.with_memory_space_constraint(gate_trained, pltpu.HBM),
        pltpu.with_memory_space_constraint(up_trained, pltpu.HBM),
        pltpu.with_memory_space_constraint(down_trained, pltpu.HBM),
    )
    gate, up, down, mixed = pl.pallas_call(
        write_out,
        out_shape=shapes,
        in_specs=[in_vmem] * 4,
        out_specs=(hbm,) * 4,
        scratch_shapes=[dma((4,))],
        compiler_params=pltpu.CompilerParams(vmem_limit_bytes=1024 * 1024),
    )(*results)
    return gate.reshape(88, 4096).T, up.reshape(88, 4096).T, down.reshape(88, 4096), mixed.T


def solution(mesh):
    finer = Mesh(mesh.devices.reshape(8, 8, 2, mesh.shape["tp"]), AXES)
    rows = AXES[:3]
    return jax.shard_map(
        on_device,
        mesh=finer,
        in_specs=(P("tp", None), P(rows), P(rows, "tp"), P(rows, "tp"), P(rows, "tp")),
        out_specs=(P(None, rows), P(None, rows), P(rows, None), P("tp", rows)),
        check_vma=False,
    )
```

```python
import jax
import jax.numpy as jnp
from jax import lax
from jax.experimental import pallas as pl
from jax.experimental.pallas import tpu as pltpu
from jax.sharding import Mesh
from jax.sharding import PartitionSpec as P

MESH = pl.DeviceIdType.MESH
AXES = ("fz", "fy", "fc", "tp")
BF16 = jnp.bfloat16
F32 = jnp.float32
LIMIT = 40 * 1024 * 1024
FAR_FIRST = (4, 3, 5, 2, 6, 1, 7)


def remote(src, dst, send, recv, device):
    return pltpu.make_async_remote_copy(
        src_ref=src, dst_ref=dst, send_sem=send, recv_sem=recv, device_id=device, device_id_type=MESH
    )


class Flights:
    def __init__(self):
        self.all = []
        self.landed = set()

    def note(self, copy):
        self.all.append(copy)
        return copy

    def go(self, copy):
        copy.start()
        return self.note(copy)

    def land(self, copy):
        copy.wait_recv()
        self.landed.add(id(copy))

    def finish(self):
        for copy in self.all:
            if id(copy) not in self.landed:
                copy.wait_recv()
        for copy in self.all:
            copy.wait_send()


def kernel(
    tokens_hbm, gain_hbm, gate_hbm, up_hbm, down_hbm,
    gate_out, up_out, down_out, mixed_out,
    tok, gain_in, gate_in, up_in, down_in, packed, r1, r2, w, normed, tok_send, tok_all, acc, core_send, core_got, plane_send, plane_got, db, parts, got, pieces, got2, last, mix,
    in_sem, ts, tr, us, ur, vs, vr, xs, xr, as_, ar, bs, br, ds, dr, gs, gr, cs, cr, es, er, ps, pr, qs, qr, fs, fr,
):
    z, y, c, x = (lax.axis_index(a) for a in AXES)
    right, left, opposite = lax.rem(x + 1, 4), lax.rem(x + 3, 4), lax.rem(x + 2, 4)
    partner = (z, y, 1 - c, x)
    flights = Flights()
    go, land = flights.go, flights.land

    def x_peer(p):
        return (z, y, c, p)

    first = jnp.where(c == 0, y, z)
    second = jnp.where(c == 0, z, y)

    def first_peer(p):
        return (jnp.where(c == 0, z, p), jnp.where(c == 0, p, y), c, x)

    def second_peer(p):
        return (jnp.where(c == 0, p, z), jnp.where(c == 0, y, p), c, x)

    barrier = pltpu.get_barrier_semaphore()
    peers = [x_peer(lax.rem(x + k, 4)) for k in (1, 2, 3)]
    peers += [first_peer(lax.rem(first + k, 8)) for k in range(1, 8)]
    peers += [second_peer(lax.rem(second + k, 8)) for k in range(1, 8)]
    peers += [partner]
    loads = [
        pltpu.make_async_copy(gate_hbm, gate_in, in_sem.at[0]),
        pltpu.make_async_copy(up_hbm, up_in, in_sem.at[1]),
        pltpu.make_async_copy(down_hbm, down_in, in_sem.at[2]),
        pltpu.make_async_copy(tokens_hbm, tok, in_sem.at[3]),
        pltpu.make_async_copy(gain_hbm, gain_in, in_sem.at[4]),
    ]
    for load in loads:
        load.start()
    for peer in peers:
        pl.semaphore_signal(barrier, inc=1, device_id=peer, device_id_type=MESH)

    lanes = lax.broadcasted_iota(jnp.int32, (32, 32), 1)
    rows = lax.broadcasted_iota(jnp.int32, (32, 32), 0)
    loads[4].wait()
    spread = jnp.broadcast_to(gain_in[...], (32, 32))
    gain = jnp.sum(jnp.where(lanes == rows, spread, 0.0), axis=1, keepdims=True)
    loads[0].wait()
    loads[1].wait()
    for s in range(4):
        scale = gain[8 * s : 8 * s + 8]
        g = gate_in[8 * s : 8 * s + 8, :] * scale
        u = up_in[8 * s : 8 * s + 8, :] * scale
        for j in range(16):
            cut = slice(176 * j, 176 * j + 176)
            unit = jnp.concatenate([g[:, cut], u[:, cut], jnp.zeros((8, 32), F32)], axis=1).astype(BF16)
            for n in range(3):
                packed[n, s, j // 8, j % 8] = unit[:, 128 * n : 128 * n + 128]

    pl.semaphore_wait(barrier, 18)
    x_sends = []
    for n in range(3):
        x_sends.append([])
        for k in (2, 1, 3):
            p = lax.rem(x + k, 4)
            x_sends[n].append(
                go(remote(packed.at[n, p], r1.at[n, pl.ds(2 * x, 2)], xs.at[n, k], xr.at[n, k], x_peer(p)))
            )

    loads[3].wait()

    def norm_rows(i, carry):
        part = tok[pl.ds(pl.multiple_of(16 * i, 16), 16), :].astype(F32)
        mean = jnp.mean(part * part, axis=-1, keepdims=True)
        normed[pl.ds(pl.multiple_of(16 * i, 16), 16), :] = (part * lax.rsqrt(mean + 1e-06)).astype(BF16)
        return carry

    lax.fori_loop(0, 12, norm_rows, 0)
    at = lax.broadcasted_iota(jnp.int32, (512, 256), 0)
    to = lax.broadcasted_iota(jnp.int32, (512, 256), 1)
    source = 64 * (to % 64 // 8) + 32 * c + 8 * (to // 64) + to % 8
    pick = jnp.where(at == source, 1.0, 0.0).astype(BF16)
    for q in range(4):
        even, odd = (
            jnp.dot(normed[:, 512 * v : 512 * v + 512], pick, preferred_element_type=F32).astype(BF16)
            for v in (2 * q, 2 * q + 1)
        )
        for s in range(4):
            cut = slice(64 * s, 64 * s + 64)
            tok_send[s, :, 128 * q : 128 * q + 128] = jnp.concatenate([even[:, cut], odd[:, cut]], axis=1)
    t_sends = []
    for k in (2, 1, 3):
        p = lax.rem(x + k, 4)
        t_sends.append(go(remote(tok_send.at[p], tok_all.at[x], ts.at[k], tr.at[k], x_peer(p))))
    tok_all[x] = tok_send[x]

    loads[2].wait()
    for i in range(11):
        db[c, x, i] = down_in[8 * i : 8 * i + 8, :].astype(BF16)

    def down_copy(t, h, k, p):
        half = db.at[c, t, :, :, pl.ds(512 * h, 512)]
        return remote(half, half, ds.at[k], dr.at[k], x_peer(p))

    d_ways = [
        go(down_copy(x, 0, 0, right)), go(down_copy(x, 1, 1, left)),
        go(down_copy(x, 1, 2, right)), go(down_copy(x, 0, 3, left)),
    ]

    for n in range(3):
        r1[n, pl.ds(2 * x, 2)] = packed[n, x]

    a_sends = []
    for n in range(3):
        for send in x_sends[n]:
            land(send)
        a_sends.append([])
        for k in FAR_FIRST:
            p = lax.rem(first + k, 8)
            sems = as_.at[n, k], ar.at[n, k]

            @pl.when(c == 0)
            def _():
                remote(r1.at[n, :, p], r2.at[n, first], *sems, first_peer(p)).start()

            @pl.when(c == 1)
            def _():
                remote(r1.at[n, p], r2.at[n, first], *sems, first_peer(p)).start()

            a_sends[n].append(flights.note(remote(r1.at[n, p], r2.at[n, first], *sems, first_peer(p))))

        @pl.when(c == 0)
        def _():
            r2[n, first] = r1[n, :, first]

        @pl.when(c == 1)
        def _():
            r2[n, first] = r1[n, first]

    b_sends = []
    for n in range(3):
        for send in a_sends[n]:
            land(send)
        b_sends.append([])
        for k in FAR_FIRST:
            p = lax.rem(second + k, 8)
            sems = bs.at[n, k], br.at[n, k]

            @pl.when(c == 0)
            def _():
                remote(r2.at[n, :, p], w.at[n, second, :, c, x], *sems, second_peer(p)).start()

            @pl.when(c == 1)
            def _():
                remote(r2.at[n, :, p], w.at[n, :, second, c, x], *sems, second_peer(p)).start()

            b_sends[n].append(
                flights.note(remote(r2.at[n, :, p], w.at[n, second, :, c, x], *sems, second_peer(p)))
            )

        @pl.when(c == 0)
        def _():
            w[n, second, :, c, x] = r2[n, :, second]

        @pl.when(c == 1)
        def _():
            w[n, :, second, c, x] = r2[n, :, second]

    def gather_copy(s, n, h, k, p):
        half = w.at[n, :, pl.ds(4 * h, 4), c, s]
        return remote(half, half, gs.at[n, k], gr.at[n, k], x_peer(p))

    def core_copy(s, n, k):
        return remote(w.at[n, :, :, c, s], w.at[n, :, :, c, s], cs.at[n, k], cr.at[n, k], partner)

    for send in t_sends:
        land(send)
    u_sends = []
    for n in range(3):
        for send in b_sends[n]:
            land(send)
        part = jnp.dot(
            tok_all[...].reshape(768, 512), w[n, :, :, c, x].reshape(512, 128), preferred_element_type=F32
        ).reshape(4, 2, 96, 128)
        acc[n] = part

        @pl.when(c == 0)
        def _():
            core_send[n] = part[:, 1].astype(BF16)

        @pl.when(c == 1)
        def _():
            core_send[n] = part[:, 0].astype(BF16)

        u_sends.append(go(remote(core_send.at[n], core_got.at[n], us.at[n], ur.at[n], partner)))
        if n == 0:
            land(d_ways[0])
            d_ways.append(go(down_copy(left, 0, 4, right)))
            land(d_ways[1])
            d_ways.append(go(down_copy(right, 1, 5, left)))
    v_sends = []
    for n in range(3):
        land(u_sends[n])
        plane_send[n] = (acc[n, :, c] + core_got[n].astype(F32)).astype(BF16)
        v_sends.append([])
        for k in (2, 1, 3):
            p = lax.rem(x + k, 4)
            v_sends[n].append(
                go(remote(plane_send.at[n, p], plane_got.at[n, x], vs.at[n, k], vr.at[n, k], x_peer(p)))
            )
    for send in d_ways[2:]:
        land(send)
    whole = go(remote(db.at[c], db.at[c], es, er, partner))
    ways = []
    swaps = []
    for n in range(3):
        ways.append([
            go(gather_copy(x, n, 0, 0, right)), go(gather_copy(x, n, 1, 1, left)),
            go(gather_copy(x, n, 1, 2, right)), go(gather_copy(x, n, 0, 3, left)),
        ])
        swaps.append([go(core_copy(x, n, 0))])
    sums = []
    for n in range(3):
        for send in v_sends[n]:
            land(send)
        total = acc[n, x, c] + core_got[n, x].astype(F32)
        for k in (1, 2, 3):
            total += plane_got[n, lax.rem(x + k, 4)].astype(F32)
        sums.append(total)
    gate = jnp.concatenate([sums[0], sums[1][:, :48]], axis=1)
    up = jnp.concatenate([sums[1][:, 48:], sums[2][:, :96]], axis=1)
    hidden = (gate * (1.0 / (1.0 + jnp.exp(-gate))) * up).astype(BF16)
    land(whole)

    @pl.when(c == 0)
    def _():
        for p in range(8):
            cols = [
                db[:, q // 2, :, :, 512 * (q % 2) + 64 * p : 512 * (q % 2) + 64 * p + 64].reshape(176, 64)
                for q in range(8)
            ]
            parts[p] = jnp.dot(hidden, jnp.concatenate(cols, axis=1), preferred_element_type=F32).astype(BF16)

    @pl.when(c == 1)
    def _():
        for p in range(8):
            cols = db[:, p // 2, :, :, 512 * (p % 2) : 512 * (p % 2) + 512].reshape(176, 512)
            parts[p] = jnp.dot(hidden, cols, preferred_element_type=F32).astype(BF16)

    p_sends = []
    for k in FAR_FIRST:
        p = lax.rem(first + k, 8)
        p_sends.append(go(remote(parts.at[p], got.at[first], ps.at[k], pr.at[k], first_peer(p))))

    for t in range(4):
        down_out[:, :, 1024 * t : 1024 * t + 1024] = db[c, t]
    for n in range(3):
        land(ways[n][0])
        ways[n].append(go(gather_copy(left, n, 0, 4, right)))
        land(ways[n][1])
        ways[n].append(go(gather_copy(right, n, 1, 5, left)))
        land(ways[n][2])
        swaps[n].append(go(core_copy(left, n, 1)))
        land(ways[n][3])
        swaps[n].append(go(core_copy(right, n, 2)))

    for send in p_sends:
        land(send)
    total = parts[first].astype(F32)
    for k in FAR_FIRST:
        total += got[lax.rem(first + k, 8)].astype(F32)
    for q in range(8):
        both = jnp.concatenate([total[:48, 64 * q : 64 * q + 64], total[48:, 64 * q : 64 * q + 64]], axis=1)
        pieces[q] = both.astype(BF16)
    q_sends = []
    for k in FAR_FIRST:
        p = lax.rem(second + k, 8)
        q_sends.append(go(remote(pieces.at[p], got2.at[second], qs.at[k], qr.at[k], second_peer(p))))
    for n in range(3):
        land(ways[n][4])
        land(ways[n][5])
        swaps[n].append(go(core_copy(opposite, n, 3)))
    for n in range(3):
        for send in swaps[n]:
            land(send)
        for core in range(2):
            @pl.when(c == core)
            def _():
                def unpack(i, carry):
                    at = pl.ds(pl.multiple_of(512 * i, 512), 512)
                    tile = w[n, i].reshape(512, 128).T
                    for out, start in ((gate_out, 88 * core), (up_out, 176 + 88 * core)):
                        for r in range(11):
                            k = start + 8 * r - 128 * n
                            if 0 <= k < 128:
                                out[r, :, at] = tile[k : k + 8]
                    return carry

                lax.fori_loop(0, 8, unpack, 0)
    for send in q_sends:
        land(send)
    total = pieces[second].astype(F32)
    for k in FAR_FIRST:
        total += got2[lax.rem(second + k, 8)].astype(F32)
    total = jnp.concatenate([total[:, :64], total[:, 64:]], axis=0)

    @pl.when(c == 0)
    def _():
        mix[c] = total[:, :32].astype(BF16)
        last[...] = total[:, 32:].astype(BF16)

    @pl.when(c == 1)
    def _():
        mix[c] = total[:, 32:].astype(BF16)
        last[...] = total[:, :32].astype(BF16)

    land(go(remote(last, mix.at[c], fs, fr, partner)))
    mixed_out[...] = jnp.concatenate([mix[0], mix[1]], axis=0).astype(F32).T.astype(BF16)
    flights.finish()


def write_out(*refs):
    sem = refs[-1]
    copies = [pltpu.make_async_copy(refs[k], refs[k + 4], sem.at[k]) for k in range(4)]
    for copy in copies:
        copy.start()
    for copy in copies:
        copy.wait()


def on_device(prompt_tokens, norm_gain, gate_trained, up_trained, down_trained):
    dma = pltpu.SemaphoreType.DMA
    hbm = pl.BlockSpec(memory_space=pltpu.HBM)
    in_vmem = pl.BlockSpec(memory_space=pltpu.VMEM)
    vmem = pltpu.VMEM
    shapes = (
        jax.ShapeDtypeStruct((11, 8, 4096), BF16),
        jax.ShapeDtypeStruct((11, 8, 4096), BF16),
        jax.ShapeDtypeStruct((11, 8, 4096), BF16),
        jax.ShapeDtypeStruct((32, 192), BF16),
    )
    results = pl.pallas_call(
        kernel,
        out_shape=[pltpu.VMEM(a.shape, a.dtype) for a in shapes],
        in_specs=[hbm] * 5,
        out_specs=(in_vmem,) * 4,
        scratch_shapes=[
            vmem((192, 4096), BF16),
            vmem((1, 32), F32),
            vmem((32, 2816), F32),
            vmem((32, 2816), F32),
            vmem((88, 1024), F32),
            vmem((3, 4, 2, 8, 8, 128), BF16),
            vmem((3, 8, 8, 8, 128), BF16),
            vmem((3, 8, 8, 8, 128), BF16),
            vmem((3, 8, 8, 2, 4, 8, 128), BF16),
            vmem((192, 4096), BF16),
            vmem((4, 192, 512), BF16),
            vmem((4, 192, 512), BF16),
            vmem((3, 4, 2, 96, 128), F32),
            vmem((3, 4, 96, 128), BF16),
            vmem((3, 4, 96, 128), BF16),
            vmem((3, 4, 96, 128), BF16),
            vmem((3, 4, 96, 128), BF16),
            vmem((2, 4, 11, 8, 1024), BF16),
            vmem((8, 96, 512), BF16),
            vmem((8, 96, 512), BF16),
            vmem((8, 48, 128), BF16),
            vmem((8, 48, 128), BF16),
            vmem((96, 32), BF16),
            vmem((2, 96, 32), BF16),
            dma((5,)),
            dma((4,)), dma((4,)),
            dma((3,)), dma((3,)),
            dma((3, 4)), dma((3, 4)),
            dma((3, 4)), dma((3, 4)),
            dma((3, 8)), dma((3, 8)),
            dma((3, 8)), dma((3, 8)),
            dma((6,)), dma((6,)),
            dma((3, 6)), dma((3, 6)),
            dma((3, 4)), dma((3, 4)),
            dma, dma,
            dma((8,)), dma((8,)),
            dma((8,)), dma((8,)),
            dma, dma,
        ],
        compiler_params=pltpu.CompilerParams(
            collective_id=0, has_side_effects=True, vmem_limit_bytes=LIMIT
        ),
    )(
        pltpu.with_memory_space_constraint(prompt_tokens, pltpu.HBM),
        pltpu.with_memory_space_constraint(norm_gain.reshape(1, 32), pltpu.HBM),
        pltpu.with_memory_space_constraint(gate_trained, pltpu.HBM),
        pltpu.with_memory_space_constraint(up_trained, pltpu.HBM),
        pltpu.with_memory_space_constraint(down_trained, pltpu.HBM),
    )
    gate, up, down, mixed = pl.pallas_call(
        write_out,
        out_shape=shapes,
        in_specs=[in_vmem] * 4,
        out_specs=(hbm,) * 4,
        scratch_shapes=[dma((4,))],
        compiler_params=pltpu.CompilerParams(vmem_limit_bytes=1024 * 1024),
    )(*results)
    return gate.reshape(88, 4096).T, up.reshape(88, 4096).T, down.reshape(88, 4096), mixed.T


def solution(mesh):
    finer = Mesh(mesh.devices.reshape(8, 8, 2, mesh.shape["tp"]), AXES)
    rows = AXES[:3]
    return jax.shard_map(
        on_device,
        mesh=finer,
        in_specs=(P("tp", None), P(rows), P(rows, "tp"), P(rows, "tp"), P(rows, "tp")),
        out_specs=(P(None, rows), P(None, rows), P(rows, None), P("tp", rows)),
        check_vma=False,
    )
```

```python
import jax
import jax.numpy as jnp
from jax import lax
from jax.experimental import pallas as pl
from jax.experimental.pallas import tpu as pltpu
from jax.sharding import Mesh
from jax.sharding import PartitionSpec as P

MESH = pl.DeviceIdType.MESH
AXES = ("fz", "fy", "fc", "tp")
BF16 = jnp.bfloat16
F32 = jnp.float32
LIMIT = 40 * 1024 * 1024
FAR_FIRST = (4, 3, 5, 2, 6, 1, 7)


def remote(src, dst, send, recv, device):
    return pltpu.make_async_remote_copy(
        src_ref=src, dst_ref=dst, send_sem=send, recv_sem=recv, device_id=device, device_id_type=MESH
    )


class Flights:
    def __init__(self):
        self.all = []
        self.landed = set()

    def note(self, copy):
        self.all.append(copy)
        return copy

    def go(self, copy):
        copy.start()
        return self.note(copy)

    def land(self, copy):
        copy.wait_recv()
        self.landed.add(id(copy))

    def finish(self):
        for copy in self.all:
            if id(copy) not in self.landed:
                copy.wait_recv()
        for copy in self.all:
            copy.wait_send()


def kernel(
    tokens_hbm, gain_hbm, gate_hbm, up_hbm, down_hbm,
    gate_out, up_out, down_out, mixed_out,
    tok, gain_in, gate_in, up_in, down_in, packed, r1, r2, w, normed, tok_send, tok_all, acc, core_send, core_got, plane_send, plane_got, db, cols_of, parts, got, pieces, got2,
    in_sem, ts, tr, us, ur, vs, vr, xs, xr, as_, ar, bs, br, ds, dr, gs, gr, cs, cr, es, er, ps, pr, qs, qr,
):
    z, y, c, x = (lax.axis_index(a) for a in AXES)
    right, left, opposite = lax.rem(x + 1, 4), lax.rem(x + 3, 4), lax.rem(x + 2, 4)
    partner = (z, y, 1 - c, x)
    flights = Flights()
    go, land = flights.go, flights.land

    def x_peer(p):
        return (z, y, c, p)

    first = jnp.where(c == 0, y, z)
    second = jnp.where(c == 0, z, y)

    def first_peer(p):
        return (jnp.where(c == 0, z, p), jnp.where(c == 0, p, y), c, x)

    def second_peer(p):
        return (jnp.where(c == 0, p, z), jnp.where(c == 0, y, p), c, x)

    def other_core(device):
        return device[0], device[1], 1 - c, x

    barrier = pltpu.get_barrier_semaphore()
    peers = [x_peer(lax.rem(x + k, 4)) for k in (1, 2, 3)]
    peers += [first_peer(lax.rem(first + k, 8)) for k in range(1, 8)]
    peers += [second_peer(lax.rem(second + k, 8)) for k in range(1, 8)]
    peers += [partner]
    peers += [other_core(second_peer(lax.rem(second + k, 8))) for k in range(1, 8)]
    peers += [other_core(first_peer(lax.rem(first + k, 8))) for k in range(1, 8)]
    loads = [
        pltpu.make_async_copy(gate_hbm, gate_in, in_sem.at[0]),
        pltpu.make_async_copy(up_hbm, up_in, in_sem.at[1]),
        pltpu.make_async_copy(down_hbm, down_in, in_sem.at[2]),
        pltpu.make_async_copy(tokens_hbm, tok, in_sem.at[3]),
        pltpu.make_async_copy(gain_hbm, gain_in, in_sem.at[4]),
    ]
    for load in loads:
        load.start()
    for peer in peers:
        pl.semaphore_signal(barrier, inc=1, device_id=peer, device_id_type=MESH)

    lanes = lax.broadcasted_iota(jnp.int32, (32, 32), 1)
    rows = lax.broadcasted_iota(jnp.int32, (32, 32), 0)
    loads[4].wait()
    spread = jnp.broadcast_to(gain_in[...], (32, 32))
    gain = jnp.sum(jnp.where(lanes == rows, spread, 0.0), axis=1, keepdims=True)
    loads[0].wait()
    loads[1].wait()
    for s in range(4):
        scale = gain[8 * s : 8 * s + 8]
        g = gate_in[8 * s : 8 * s + 8, :] * scale
        u = up_in[8 * s : 8 * s + 8, :] * scale
        for j in range(16):
            cut = slice(176 * j, 176 * j + 176)
            unit = jnp.concatenate([g[:, cut], u[:, cut], jnp.zeros((8, 32), F32)], axis=1).astype(BF16)
            for n in range(3):
                packed[n, s, j // 8, j % 8] = unit[:, 128 * n : 128 * n + 128]

    pl.semaphore_wait(barrier, 32)
    x_sends = []
    for n in range(3):
        x_sends.append([])
        for k in (2, 1, 3):
            p = lax.rem(x + k, 4)
            x_sends[n].append(
                go(remote(packed.at[n, p], r1.at[n, pl.ds(2 * x, 2)], xs.at[n, k], xr.at[n, k], x_peer(p)))
            )

    loads[3].wait()

    def norm_rows(i, carry):
        part = tok[pl.ds(pl.multiple_of(16 * i, 16), 16), :].astype(F32)
        mean = jnp.mean(part * part, axis=-1, keepdims=True)
        normed[pl.ds(pl.multiple_of(16 * i, 16), 16), :] = (part * lax.rsqrt(mean + 1e-06)).astype(BF16)
        return carry

    lax.fori_loop(0, 12, norm_rows, 0)
    at = lax.broadcasted_iota(jnp.int32, (512, 256), 0)
    to = lax.broadcasted_iota(jnp.int32, (512, 256), 1)
    source = 64 * (to % 64 // 8) + 32 * c + 8 * (to // 64) + to % 8
    pick = jnp.where(at == source, 1.0, 0.0).astype(BF16)
    for q in range(4):
        even, odd = (
            jnp.dot(normed[:, 512 * v : 512 * v + 512], pick, preferred_element_type=F32).astype(BF16)
            for v in (2 * q, 2 * q + 1)
        )
        for s in range(4):
            cut = slice(64 * s, 64 * s + 64)
            tok_send[s, :, 128 * q : 128 * q + 128] = jnp.concatenate([even[:, cut], odd[:, cut]], axis=1)
    t_sends = []
    for k in (2, 1, 3):
        p = lax.rem(x + k, 4)
        t_sends.append(go(remote(tok_send.at[p], tok_all.at[x], ts.at[k], tr.at[k], x_peer(p))))
    tok_all[x] = tok_send[x]

    loads[2].wait()
    for i in range(11):
        db[c, x, i] = down_in[8 * i : 8 * i + 8, :].astype(BF16)

    def down_copy(t, h, k, p):
        half = db.at[c, t, :, :, pl.ds(512 * h, 512)]
        return remote(half, half, ds.at[k], dr.at[k], x_peer(p))

    d_ways = [
        go(down_copy(x, 0, 0, right)), go(down_copy(x, 1, 1, left)),
        go(down_copy(x, 1, 2, right)), go(down_copy(x, 0, 3, left)),
    ]

    for n in range(3):
        r1[n, pl.ds(2 * x, 2)] = packed[n, x]

    a_sends = []
    for n in range(3):
        for send in x_sends[n]:
            land(send)
        a_sends.append([])
        for k in FAR_FIRST:
            p = lax.rem(first + k, 8)
            sems = as_.at[n, k], ar.at[n, k]

            @pl.when(c == 0)
            def _():
                remote(r1.at[n, :, p], r2.at[n, first], *sems, first_peer(p)).start()

            @pl.when(c == 1)
            def _():
                remote(r1.at[n, p], r2.at[n, first], *sems, first_peer(p)).start()

            a_sends[n].append(flights.note(remote(r1.at[n, p], r2.at[n, first], *sems, first_peer(p))))

        @pl.when(c == 0)
        def _():
            r2[n, first] = r1[n, :, first]

        @pl.when(c == 1)
        def _():
            r2[n, first] = r1[n, first]

    b_sends = []
    for n in range(3):
        for send in a_sends[n]:
            land(send)
        b_sends.append([])
        for k in FAR_FIRST:
            p = lax.rem(second + k, 8)
            sems = bs.at[n, k], br.at[n, k]

            @pl.when(c == 0)
            def _():
                remote(r2.at[n, :, p], w.at[n, second, :, c, x], *sems, second_peer(p)).start()

            @pl.when(c == 1)
            def _():
                remote(r2.at[n, :, p], w.at[n, :, second, c, x], *sems, second_peer(p)).start()

            b_sends[n].append(
                flights.note(remote(r2.at[n, :, p], w.at[n, second, :, c, x], *sems, second_peer(p)))
            )

        @pl.when(c == 0)
        def _():
            w[n, second, :, c, x] = r2[n, :, second]

        @pl.when(c == 1)
        def _():
            w[n, :, second, c, x] = r2[n, :, second]

    def gather_copy(s, n, h, k, p):
        half = w.at[n, :, pl.ds(4 * h, 4), c, s]
        return remote(half, half, gs.at[n, k], gr.at[n, k], x_peer(p))

    def core_copy(s, n, k):
        return remote(w.at[n, :, :, c, s], w.at[n, :, :, c, s], cs.at[n, k], cr.at[n, k], partner)

    for send in t_sends:
        land(send)
    u_sends = []
    for n in range(3):
        for send in b_sends[n]:
            land(send)
        part = jnp.dot(
            tok_all[...].reshape(768, 512), w[n, :, :, c, x].reshape(512, 128), preferred_element_type=F32
        ).reshape(4, 2, 96, 128)
        acc[n] = part

        @pl.when(c == 0)
        def _():
            core_send[n] = part[:, 1].astype(BF16)

        @pl.when(c == 1)
        def _():
            core_send[n] = part[:, 0].astype(BF16)

        u_sends.append(go(remote(core_send.at[n], core_got.at[n], us.at[n], ur.at[n], partner)))
        if n == 0:
            land(d_ways[0])
            d_ways.append(go(down_copy(left, 0, 4, right)))
            land(d_ways[1])
            d_ways.append(go(down_copy(right, 1, 5, left)))
    v_sends = []
    for n in range(3):
        land(u_sends[n])
        plane_send[n] = (acc[n, :, c] + core_got[n].astype(F32)).astype(BF16)
        v_sends.append([])
        for k in (2, 1, 3):
            p = lax.rem(x + k, 4)
            v_sends[n].append(
                go(remote(plane_send.at[n, p], plane_got.at[n, x], vs.at[n, k], vr.at[n, k], x_peer(p)))
            )
    for send in d_ways[2:]:
        land(send)
    whole = go(remote(db.at[c], db.at[c], es, er, partner))
    ways = []
    swaps = []
    for n in range(3):
        ways.append([
            go(gather_copy(x, n, 0, 0, right)), go(gather_copy(x, n, 1, 1, left)),
            go(gather_copy(x, n, 1, 2, right)), go(gather_copy(x, n, 0, 3, left)),
        ])
        swaps.append([go(core_copy(x, n, 0))])
    land(whole)

    @pl.when(c == 0)
    def _():
        for p in range(8):
            cols = [
                db[:, q // 2, :, :, 512 * (q % 2) + 64 * p : 512 * (q % 2) + 64 * p + 64].reshape(176, 64)
                for q in range(8)
            ]
            cols_of[p] = jnp.concatenate(cols, axis=1)

    @pl.when(c == 1)
    def _():
        for p in range(8):
            cols_of[p] = db[:, p // 2, :, :, 512 * (p % 2) : 512 * (p % 2) + 512].reshape(176, 512)

    sums = []
    for n in range(3):
        for send in v_sends[n]:
            land(send)
        total = acc[n, x, c] + core_got[n, x].astype(F32)
        for k in (1, 2, 3):
            total += plane_got[n, lax.rem(x + k, 4)].astype(F32)
        sums.append(total)
    gate = jnp.concatenate([sums[0], sums[1][:, :48]], axis=1)
    up = jnp.concatenate([sums[1][:, 48:], sums[2][:, :96]], axis=1)
    hidden = (gate * (1.0 / (1.0 + jnp.exp(-gate))) * up).astype(BF16)

    p_sends = []
    for k in (*FAR_FIRST, 0):
        p = lax.rem(first + k, 8)
        parts[p] = jnp.dot(hidden, cols_of[p], preferred_element_type=F32).astype(BF16)
        if k:
            p_sends.append(go(remote(parts.at[p], got.at[first], ps.at[k], pr.at[k], first_peer(p))))

    for t in range(4):
        down_out[:, :, 1024 * t : 1024 * t + 1024] = db[c, t]
    for n in range(3):
        land(ways[n][0])
        ways[n].append(go(gather_copy(left, n, 0, 4, right)))
        land(ways[n][1])
        ways[n].append(go(gather_copy(right, n, 1, 5, left)))
        land(ways[n][2])
        swaps[n].append(go(core_copy(left, n, 1)))
        land(ways[n][3])
        swaps[n].append(go(core_copy(right, n, 2)))

    q_sends = []
    total = parts[first].astype(F32)
    for k, send in zip(FAR_FIRST, p_sends):
        land(send)
        total += got[lax.rem(first + 8 - k, 8)].astype(F32)
    for q in range(16):
        groups = [total[32 * g : 32 * g + 32, 32 * q : 32 * q + 32] for g in range(3)]
        block = jnp.concatenate(groups + [jnp.zeros((32, 32), F32)], axis=1)
        pieces[q // 2, q % 2] = block.astype(BF16)
    for k in (*FAR_FIRST, 0):
        p = lax.rem(second + k, 8)
        for other in range(2):
            if k or other:
                d = 1 - c if other else c
                device = other_core(second_peer(p)) if other else second_peer(p)
                sems = qs.at[other, k], qr.at[other, k]
                q_sends.append(go(remote(pieces.at[p, d], got2.at[c, second], *sems, device)))
    got2[c, second] = pieces[second, c]
    for n in range(3):
        land(ways[n][4])
        land(ways[n][5])
        swaps[n].append(go(core_copy(opposite, n, 3)))
    for n in range(3):
        for send in swaps[n]:
            land(send)
        for core in range(2):
            @pl.when(c == core)
            def _():
                def unpack(i, carry):
                    at = pl.ds(pl.multiple_of(512 * i, 512), 512)
                    tile = w[n, i].reshape(512, 128).T
                    for out, start in ((gate_out, 88 * core), (up_out, 176 + 88 * core)):
                        for r in range(11):
                            k = start + 8 * r - 128 * n
                            if 0 <= k < 128:
                                out[r, :, at] = tile[k : k + 8]
                    return carry

                lax.fori_loop(0, 8, unpack, 0)
    for send in q_sends:
        land(send)
    blocks = []
    for core in range(2):
        total = got2[core, 0].astype(F32)
        for q in range(1, 8):
            total += got2[core, q].astype(F32)
        blocks += [total[:, 32 * g : 32 * g + 32] for g in range(3)]
    mixed_out[...] = jnp.concatenate(blocks, axis=0).T.astype(BF16)
    flights.finish()


def write_out(*refs):
    sem = refs[-1]
    copies = [pltpu.make_async_copy(refs[k], refs[k + 4], sem.at[k]) for k in range(4)]
    for copy in copies:
        copy.start()
    for copy in copies:
        copy.wait()


def on_device(prompt_tokens, norm_gain, gate_trained, up_trained, down_trained):
    dma = pltpu.SemaphoreType.DMA
    hbm = pl.BlockSpec(memory_space=pltpu.HBM)
    in_vmem = pl.BlockSpec(memory_space=pltpu.VMEM)
    vmem = pltpu.VMEM
    shapes = (
        jax.ShapeDtypeStruct((11, 8, 4096), BF16),
        jax.ShapeDtypeStruct((11, 8, 4096), BF16),
        jax.ShapeDtypeStruct((11, 8, 4096), BF16),
        jax.ShapeDtypeStruct((32, 192), BF16),
    )
    results = pl.pallas_call(
        kernel,
        out_shape=[pltpu.VMEM(a.shape, a.dtype) for a in shapes],
        in_specs=[hbm] * 5,
        out_specs=(in_vmem,) * 4,
        scratch_shapes=[
            vmem((192, 4096), BF16),
            vmem((1, 32), F32),
            vmem((32, 2816), F32),
            vmem((32, 2816), F32),
            vmem((88, 1024), F32),
            vmem((3, 4, 2, 8, 8, 128), BF16),
            vmem((3, 8, 8, 8, 128), BF16),
            vmem((3, 8, 8, 8, 128), BF16),
            vmem((3, 8, 8, 2, 4, 8, 128), BF16),
            vmem((192, 4096), BF16),
            vmem((4, 192, 512), BF16),
            vmem((4, 192, 512), BF16),
            vmem((3, 4, 2, 96, 128), F32),
            vmem((3, 4, 96, 128), BF16),
            vmem((3, 4, 96, 128), BF16),
            vmem((3, 4, 96, 128), BF16),
            vmem((3, 4, 96, 128), BF16),
            vmem((2, 4, 11, 8, 1024), BF16),
            vmem((8, 176, 512), BF16),
            vmem((8, 96, 512), BF16),
            vmem((8, 96, 512), BF16),
            vmem((8, 2, 32, 128), BF16),
            vmem((2, 8, 32, 128), BF16),
            dma((5,)),
            dma((4,)), dma((4,)),
            dma((3,)), dma((3,)),
            dma((3, 4)), dma((3, 4)),
            dma((3, 4)), dma((3, 4)),
            dma((3, 8)), dma((3, 8)),
            dma((3, 8)), dma((3, 8)),
            dma((6,)), dma((6,)),
            dma((3, 6)), dma((3, 6)),
            dma((3, 4)), dma((3, 4)),
            dma, dma,
            dma((8,)), dma((8,)),
            dma((2, 8)), dma((2, 8)),
        ],
        compiler_params=pltpu.CompilerParams(
            collective_id=0, has_side_effects=True, vmem_limit_bytes=LIMIT
        ),
    )(
        pltpu.with_memory_space_constraint(prompt_tokens, pltpu.HBM),
        pltpu.with_memory_space_constraint(norm_gain.reshape(1, 32), pltpu.HBM),
        pltpu.with_memory_space_constraint(gate_trained, pltpu.HBM),
        pltpu.with_memory_space_constraint(up_trained, pltpu.HBM),
        pltpu.with_memory_space_constraint(down_trained, pltpu.HBM),
    )
    gate, up, down, mixed = pl.pallas_call(
        write_out,
        out_shape=shapes,
        in_specs=[in_vmem] * 4,
        out_specs=(hbm,) * 4,
        scratch_shapes=[dma((4,))],
        compiler_params=pltpu.CompilerParams(vmem_limit_bytes=1024 * 1024),
    )(*results)
    return gate.reshape(88, 4096).T, up.reshape(88, 4096).T, down.reshape(88, 4096), mixed.T


def solution(mesh):
    finer = Mesh(mesh.devices.reshape(8, 8, 2, mesh.shape["tp"]), AXES)
    rows = AXES[:3]
    return jax.shard_map(
        on_device,
        mesh=finer,
        in_specs=(P("tp", None), P(rows), P(rows, "tp"), P(rows, "tp"), P(rows, "tp")),
        out_specs=(P(None, rows), P(None, rows), P(rows, None), P("tp", rows)),
        check_vma=False,
    )
```

```python
import jax
import jax.numpy as jnp
from jax import lax
from jax.experimental import pallas as pl
from jax.experimental.pallas import tpu as pltpu
from jax.sharding import Mesh
from jax.sharding import PartitionSpec as P

MESH = pl.DeviceIdType.MESH
AXES = ("fz", "fy", "fc", "tp")
BF16 = jnp.bfloat16
F32 = jnp.float32
LIMIT = 40 * 1024 * 1024
FAR_FIRST = (4, 3, 5, 2, 6, 1, 7)


def remote(src, dst, send, recv, device):
    return pltpu.make_async_remote_copy(
        src_ref=src, dst_ref=dst, send_sem=send, recv_sem=recv, device_id=device, device_id_type=MESH
    )


class Flights:
    def __init__(self):
        self.all = []
        self.landed = set()

    def note(self, copy):
        self.all.append(copy)
        return copy

    def go(self, copy):
        copy.start()
        return self.note(copy)

    def land(self, copy):
        copy.wait_recv()
        self.landed.add(id(copy))

    def finish(self):
        for copy in self.all:
            if id(copy) not in self.landed:
                copy.wait_recv()
        for copy in self.all:
            copy.wait_send()


def kernel(
    tokens_hbm, gain_hbm, gate_hbm, up_hbm, down_hbm,
    gate_out, up_out, down_out, mixed_out,
    tok, gain_in, gate_in, up_in, down_in, packed, r1, r2, w, normed, tok_send, tok_all, acc, core_send, core_got, plane_send, plane_got, db, cols_of, parts, got, pieces, got2,
    in_sem, ts, tr, us, ur, vs, vr, xs, xr, as_, ar, bs, br, ds, dr, gs, gr, cs, cr, es, er, ps, pr, qs, qr,
):
    z, y, c, x = (lax.axis_index(a) for a in AXES)
    right, left, opposite = lax.rem(x + 1, 4), lax.rem(x + 3, 4), lax.rem(x + 2, 4)
    partner = (z, y, 1 - c, x)
    flights = Flights()
    go, land = flights.go, flights.land

    def x_peer(p):
        return (z, y, c, p)

    first = jnp.where(c == 0, y, z)
    second = jnp.where(c == 0, z, y)

    def first_peer(p):
        return (jnp.where(c == 0, z, p), jnp.where(c == 0, p, y), c, x)

    def second_peer(p):
        return (jnp.where(c == 0, p, z), jnp.where(c == 0, y, p), c, x)

    def other_core(device):
        return device[0], device[1], 1 - c, x

    barrier = pltpu.get_barrier_semaphore()
    peers = [x_peer(lax.rem(x + k, 4)) for k in (1, 2, 3)]
    peers += [first_peer(lax.rem(first + k, 8)) for k in range(1, 8)]
    peers += [second_peer(lax.rem(second + k, 8)) for k in range(1, 8)]
    peers += [partner]
    peers += [other_core(second_peer(lax.rem(second + k, 8))) for k in range(1, 8)]
    peers += [other_core(first_peer(lax.rem(first + k, 8))) for k in range(1, 8)]
    loads = [
        pltpu.make_async_copy(gate_hbm, gate_in, in_sem.at[0]),
        pltpu.make_async_copy(up_hbm, up_in, in_sem.at[1]),
        pltpu.make_async_copy(down_hbm, down_in, in_sem.at[2]),
        pltpu.make_async_copy(tokens_hbm, tok, in_sem.at[3]),
        pltpu.make_async_copy(gain_hbm, gain_in, in_sem.at[4]),
    ]
    for k in (0, 4, 1):
        loads[k].start()
    for peer in peers:
        pl.semaphore_signal(barrier, inc=1, device_id=peer, device_id_type=MESH)

    lanes = lax.broadcasted_iota(jnp.int32, (32, 32), 1)
    rows = lax.broadcasted_iota(jnp.int32, (32, 32), 0)
    loads[4].wait()
    spread = jnp.broadcast_to(gain_in[...], (32, 32))
    gain = jnp.sum(jnp.where(lanes == rows, spread, 0.0), axis=1, keepdims=True)
    loads[0].wait()
    loads[2].start()
    loads[3].start()

    def scaled(ref, s):
        return ref[8 * s : 8 * s + 8, :] * gain[8 * s : 8 * s + 8]

    x_sends = []
    for n in range(3):
        if n == 1:
            loads[1].wait()
        for s in range(4):
            g = scaled(gate_in, s) if n < 2 else None
            u = scaled(up_in, s) if n > 0 else None
            for j in range(16):
                at = 176 * j
                if n == 0:
                    tile = g[:, at : at + 128]
                elif n == 1:
                    tile = jnp.concatenate([g[:, at + 128 : at + 176], u[:, at : at + 80]], axis=1)
                else:
                    tile = jnp.concatenate([u[:, at + 80 : at + 176], jnp.zeros((8, 32), F32)], axis=1)
                packed[n, s, j // 8, j % 8] = tile.astype(BF16)
        if n == 0:
            pl.semaphore_wait(barrier, 32)
        x_sends.append([])
        for k in (2, 1, 3):
            p = lax.rem(x + k, 4)
            x_sends[n].append(
                go(remote(packed.at[n, p], r1.at[n, pl.ds(2 * x, 2)], xs.at[n, k], xr.at[n, k], x_peer(p)))
            )

    loads[3].wait()

    def norm_rows(i, carry):
        part = tok[pl.ds(pl.multiple_of(16 * i, 16), 16), :].astype(F32)
        mean = jnp.mean(part * part, axis=-1, keepdims=True)
        normed[pl.ds(pl.multiple_of(16 * i, 16), 16), :] = (part * lax.rsqrt(mean + 1e-06)).astype(BF16)
        return carry

    lax.fori_loop(0, 12, norm_rows, 0)
    at = lax.broadcasted_iota(jnp.int32, (512, 256), 0)
    to = lax.broadcasted_iota(jnp.int32, (512, 256), 1)
    source = 64 * (to % 64 // 8) + 32 * c + 8 * (to // 64) + to % 8
    pick = jnp.where(at == source, 1.0, 0.0).astype(BF16)
    for q in range(4):
        even, odd = (
            jnp.dot(normed[:, 512 * v : 512 * v + 512], pick, preferred_element_type=F32).astype(BF16)
            for v in (2 * q, 2 * q + 1)
        )
        for s in range(4):
            cut = slice(64 * s, 64 * s + 64)
            tok_send[s, :, 128 * q : 128 * q + 128] = jnp.concatenate([even[:, cut], odd[:, cut]], axis=1)
    t_sends = []
    for k in (2, 1, 3):
        p = lax.rem(x + k, 4)
        t_sends.append(go(remote(tok_send.at[p], tok_all.at[x], ts.at[k], tr.at[k], x_peer(p))))
    tok_all[x] = tok_send[x]

    loads[2].wait()
    for i in range(11):
        db[c, x, i] = down_in[8 * i : 8 * i + 8, :].astype(BF16)

    def down_copy(t, h, k, p):
        half = db.at[c, t, :, :, pl.ds(512 * h, 512)]
        return remote(half, half, ds.at[k], dr.at[k], x_peer(p))

    d_ways = [
        go(down_copy(x, 0, 0, right)), go(down_copy(x, 1, 1, left)),
        go(down_copy(x, 1, 2, right)), go(down_copy(x, 0, 3, left)),
    ]

    for n in range(3):
        r1[n, pl.ds(2 * x, 2)] = packed[n, x]

    a_sends = []
    for n in range(3):
        for send in x_sends[n]:
            land(send)
        a_sends.append([])
        for k in FAR_FIRST:
            p = lax.rem(first + k, 8)
            sems = as_.at[n, k], ar.at[n, k]

            @pl.when(c == 0)
            def _():
                remote(r1.at[n, :, p], r2.at[n, first], *sems, first_peer(p)).start()

            @pl.when(c == 1)
            def _():
                remote(r1.at[n, p], r2.at[n, first], *sems, first_peer(p)).start()

            a_sends[n].append(flights.note(remote(r1.at[n, p], r2.at[n, first], *sems, first_peer(p))))

        @pl.when(c == 0)
        def _():
            r2[n, first] = r1[n, :, first]

        @pl.when(c == 1)
        def _():
            r2[n, first] = r1[n, first]

    b_sends = []
    for n in range(3):
        for send in a_sends[n]:
            land(send)
        b_sends.append([])
        for k in FAR_FIRST:
            p = lax.rem(second + k, 8)
            sems = bs.at[n, k], br.at[n, k]

            @pl.when(c == 0)
            def _():
                remote(r2.at[n, :, p], w.at[n, second, :, c, x], *sems, second_peer(p)).start()

            @pl.when(c == 1)
            def _():
                remote(r2.at[n, :, p], w.at[n, :, second, c, x], *sems, second_peer(p)).start()

            b_sends[n].append(
                flights.note(remote(r2.at[n, :, p], w.at[n, second, :, c, x], *sems, second_peer(p)))
            )

        @pl.when(c == 0)
        def _():
            w[n, second, :, c, x] = r2[n, :, second]

        @pl.when(c == 1)
        def _():
            w[n, :, second, c, x] = r2[n, :, second]

    def gather_copy(s, n, h, k, p):
        half = w.at[n, :, pl.ds(4 * h, 4), c, s]
        return remote(half, half, gs.at[n, k], gr.at[n, k], x_peer(p))

    def core_copy(s, n, k):
        return remote(w.at[n, :, :, c, s], w.at[n, :, :, c, s], cs.at[n, k], cr.at[n, k], partner)

    for send in t_sends:
        land(send)
    u_sends = []
    for n in range(3):
        for send in b_sends[n]:
            land(send)
        part = jnp.dot(
            tok_all[...].reshape(768, 512), w[n, :, :, c, x].reshape(512, 128), preferred_element_type=F32
        ).reshape(4, 2, 96, 128)
        acc[n] = part

        @pl.when(c == 0)
        def _():
            core_send[n] = part[:, 1].astype(BF16)

        @pl.when(c == 1)
        def _():
            core_send[n] = part[:, 0].astype(BF16)

        u_sends.append(go(remote(core_send.at[n], core_got.at[n], us.at[n], ur.at[n], partner)))
        if n == 0:
            land(d_ways[0])
            d_ways.append(go(down_copy(left, 0, 4, right)))
            land(d_ways[1])
            d_ways.append(go(down_copy(right, 1, 5, left)))
    v_sends = []
    for n in range(3):
        land(u_sends[n])
        plane_send[n] = (acc[n, :, c] + core_got[n].astype(F32)).astype(BF16)
        v_sends.append([])
        for k in (2, 1, 3):
            p = lax.rem(x + k, 4)
            v_sends[n].append(
                go(remote(plane_send.at[n, p], plane_got.at[n, x], vs.at[n, k], vr.at[n, k], x_peer(p)))
            )
    for send in d_ways[2:]:
        land(send)
    whole = go(remote(db.at[c], db.at[c], es, er, partner))
    ways = []
    swaps = []
    for n in range(3):
        ways.append([
            go(gather_copy(x, n, 0, 0, right)), go(gather_copy(x, n, 1, 1, left)),
            go(gather_copy(x, n, 1, 2, right)), go(gather_copy(x, n, 0, 3, left)),
        ])
        swaps.append([go(core_copy(x, n, 0))])
    land(whole)

    @pl.when(c == 0)
    def _():
        for p in range(8):
            cols = [
                db[:, q // 2, :, :, 512 * (q % 2) + 64 * p : 512 * (q % 2) + 64 * p + 64].reshape(176, 64)
                for q in range(8)
            ]
            cols_of[p] = jnp.concatenate(cols, axis=1)

    @pl.when(c == 1)
    def _():
        for p in range(8):
            cols_of[p] = db[:, p // 2, :, :, 512 * (p % 2) : 512 * (p % 2) + 512].reshape(176, 512)

    sums = []
    for n in range(3):
        for send in v_sends[n]:
            land(send)
        total = acc[n, x, c] + core_got[n, x].astype(F32)
        for k in (1, 2, 3):
            total += plane_got[n, lax.rem(x + k, 4)].astype(F32)
        sums.append(total)
    gate = jnp.concatenate([sums[0], sums[1][:, :48]], axis=1)
    up = jnp.concatenate([sums[1][:, 48:], sums[2][:, :96]], axis=1)
    hidden = (gate * (1.0 / (1.0 + jnp.exp(-gate))) * up).astype(BF16)

    p_sends = []
    for k in (*FAR_FIRST, 0):
        p = lax.rem(first + k, 8)
        parts[p] = jnp.dot(hidden, cols_of[p], preferred_element_type=F32).astype(BF16)
        if k:
            p_sends.append(go(remote(parts.at[p], got.at[first], ps.at[k], pr.at[k], first_peer(p))))

    for t in range(4):
        down_out[:, :, 1024 * t : 1024 * t + 1024] = db[c, t]
    for n in range(3):
        land(ways[n][0])
        ways[n].append(go(gather_copy(left, n, 0, 4, right)))
        land(ways[n][1])
        ways[n].append(go(gather_copy(right, n, 1, 5, left)))
        land(ways[n][2])
        swaps[n].append(go(core_copy(left, n, 1)))
        land(ways[n][3])
        swaps[n].append(go(core_copy(right, n, 2)))

    q_sends = []
    total = parts[first].astype(F32)
    for k, send in zip(FAR_FIRST, p_sends):
        land(send)
        total += got[lax.rem(first + 8 - k, 8)].astype(F32)
    for q in range(16):
        groups = [total[32 * g : 32 * g + 32, 32 * q : 32 * q + 32] for g in range(3)]
        block = jnp.concatenate(groups + [jnp.zeros((32, 32), F32)], axis=1)
        pieces[q // 2, q % 2] = block.astype(BF16)
    for k in (*FAR_FIRST, 0):
        p = lax.rem(second + k, 8)
        for other in range(2):
            if k or other:
                d = 1 - c if other else c
                device = other_core(second_peer(p)) if other else second_peer(p)
                sems = qs.at[other, k], qr.at[other, k]
                q_sends.append(go(remote(pieces.at[p, d], got2.at[c, second], *sems, device)))
    got2[c, second] = pieces[second, c]
    for n in range(3):
        land(ways[n][4])
        land(ways[n][5])
        swaps[n].append(go(core_copy(opposite, n, 3)))
    for n in range(3):
        for send in swaps[n]:
            land(send)
        for core in range(2):
            @pl.when(c == core)
            def _():
                def unpack(i, carry):
                    at = pl.ds(pl.multiple_of(512 * i, 512), 512)
                    tile = w[n, i].reshape(512, 128).T
                    for out, start in ((gate_out, 88 * core), (up_out, 176 + 88 * core)):
                        for r in range(11):
                            k = start + 8 * r - 128 * n
                            if 0 <= k < 128:
                                out[r, :, at] = tile[k : k + 8]
                    return carry

                lax.fori_loop(0, 8, unpack, 0)
    for send in q_sends:
        land(send)
    blocks = []
    for core in range(2):
        total = got2[core, 0].astype(F32)
        for q in range(1, 8):
            total += got2[core, q].astype(F32)
        blocks += [total[:, 32 * g : 32 * g + 32] for g in range(3)]
    mixed_out[...] = jnp.concatenate(blocks, axis=0).T.astype(BF16)
    flights.finish()


def write_out(*refs):
    sem = refs[-1]
    copies = [pltpu.make_async_copy(refs[k], refs[k + 4], sem.at[k]) for k in range(4)]
    for copy in copies:
        copy.start()
    for copy in copies:
        copy.wait()


def on_device(prompt_tokens, norm_gain, gate_trained, up_trained, down_trained):
    dma = pltpu.SemaphoreType.DMA
    hbm = pl.BlockSpec(memory_space=pltpu.HBM)
    in_vmem = pl.BlockSpec(memory_space=pltpu.VMEM)
    vmem = pltpu.VMEM
    shapes = (
        jax.ShapeDtypeStruct((11, 8, 4096), BF16),
        jax.ShapeDtypeStruct((11, 8, 4096), BF16),
        jax.ShapeDtypeStruct((11, 8, 4096), BF16),
        jax.ShapeDtypeStruct((32, 192), BF16),
    )
    results = pl.pallas_call(
        kernel,
        out_shape=[pltpu.VMEM(a.shape, a.dtype) for a in shapes],
        in_specs=[hbm] * 5,
        out_specs=(in_vmem,) * 4,
        scratch_shapes=[
            vmem((192, 4096), BF16),
            vmem((1, 32), F32),
            vmem((32, 2816), F32),
            vmem((32, 2816), F32),
            vmem((88, 1024), F32),
            vmem((3, 4, 2, 8, 8, 128), BF16),
            vmem((3, 8, 8, 8, 128), BF16),
            vmem((3, 8, 8, 8, 128), BF16),
            vmem((3, 8, 8, 2, 4, 8, 128), BF16),
            vmem((192, 4096), BF16),
            vmem((4, 192, 512), BF16),
            vmem((4, 192, 512), BF16),
            vmem((3, 4, 2, 96, 128), F32),
            vmem((3, 4, 96, 128), BF16),
            vmem((3, 4, 96, 128), BF16),
            vmem((3, 4, 96, 128), BF16),
            vmem((3, 4, 96, 128), BF16),
            vmem((2, 4, 11, 8, 1024), BF16),
            vmem((8, 176, 512), BF16),
            vmem((8, 96, 512), BF16),
            vmem((8, 96, 512), BF16),
            vmem((8, 2, 32, 128), BF16),
            vmem((2, 8, 32, 128), BF16),
            dma((5,)),
            dma((4,)), dma((4,)),
            dma((3,)), dma((3,)),
            dma((3, 4)), dma((3, 4)),
            dma((3, 4)), dma((3, 4)),
            dma((3, 8)), dma((3, 8)),
            dma((3, 8)), dma((3, 8)),
            dma((6,)), dma((6,)),
            dma((3, 6)), dma((3, 6)),
            dma((3, 4)), dma((3, 4)),
            dma, dma,
            dma((8,)), dma((8,)),
            dma((2, 8)), dma((2, 8)),
        ],
        compiler_params=pltpu.CompilerParams(
            collective_id=0, has_side_effects=True, vmem_limit_bytes=LIMIT
        ),
    )(
        pltpu.with_memory_space_constraint(prompt_tokens, pltpu.HBM),
        pltpu.with_memory_space_constraint(norm_gain.reshape(1, 32), pltpu.HBM),
        pltpu.with_memory_space_constraint(gate_trained, pltpu.HBM),
        pltpu.with_memory_space_constraint(up_trained, pltpu.HBM),
        pltpu.with_memory_space_constraint(down_trained, pltpu.HBM),
    )
    gate, up, down, mixed = pl.pallas_call(
        write_out,
        out_shape=shapes,
        in_specs=[in_vmem] * 4,
        out_specs=(hbm,) * 4,
        scratch_shapes=[dma((4,))],
        compiler_params=pltpu.CompilerParams(vmem_limit_bytes=1024 * 1024),
    )(*results)
    return gate.reshape(88, 4096).T, up.reshape(88, 4096).T, down.reshape(88, 4096), mixed.T


def solution(mesh):
    finer = Mesh(mesh.devices.reshape(8, 8, 2, mesh.shape["tp"]), AXES)
    rows = AXES[:3]
    return jax.shard_map(
        on_device,
        mesh=finer,
        in_specs=(P("tp", None), P(rows), P(rows, "tp"), P(rows, "tp"), P(rows, "tp")),
        out_specs=(P(None, rows), P(None, rows), P(rows, None), P("tp", rows)),
        check_vma=False,
    )
```

```python
import jax
import jax.numpy as jnp
from jax import lax
from jax.experimental import pallas as pl
from jax.experimental.pallas import tpu as pltpu
from jax.sharding import Mesh
from jax.sharding import PartitionSpec as P

MESH = pl.DeviceIdType.MESH
AXES = ("fz", "fy", "fc", "tp")
BF16 = jnp.bfloat16
F32 = jnp.float32
LIMIT = 40 * 1024 * 1024
FAR_FIRST = (4, 3, 5, 2, 6, 1, 7)


def remote(src, dst, send, recv, device):
    return pltpu.make_async_remote_copy(
        src_ref=src, dst_ref=dst, send_sem=send, recv_sem=recv, device_id=device, device_id_type=MESH
    )


class Flights:
    def __init__(self):
        self.all = []
        self.landed = set()

    def note(self, copy):
        self.all.append(copy)
        return copy

    def go(self, copy):
        copy.start()
        return self.note(copy)

    def land(self, copy):
        copy.wait_recv()
        self.landed.add(id(copy))

    def finish(self):
        for copy in self.all:
            if id(copy) not in self.landed:
                copy.wait_recv()
        for copy in self.all:
            copy.wait_send()


def kernel(
    tokens_hbm, gain_hbm, gate_hbm, up_hbm, down_hbm,
    gate_out, up_out, down_out, mixed_out,
    tok, gain_in, gate_in, up_in, down_in, packed, r1, r2, w, normed, tok_send, tok_all, acc, core_send, core_got, plane_send, plane_got, db, cols_of, parts, got, pieces, got2,
    in_sem, ts, tr, us, ur, vs, vr, xs, xr, as_, ar, bs, br, ds, dr, gs, gr, cs, cr, es, er, ps, pr, qs, qr,
):
    z, y, c, x = (lax.axis_index(a) for a in AXES)
    right, left, opposite = lax.rem(x + 1, 4), lax.rem(x + 3, 4), lax.rem(x + 2, 4)
    partner = (z, y, 1 - c, x)
    flights = Flights()
    go, land = flights.go, flights.land

    def x_peer(p):
        return (z, y, c, p)

    first = jnp.where(c == 0, y, z)
    second = jnp.where(c == 0, z, y)

    def first_peer(p):
        return (jnp.where(c == 0, z, p), jnp.where(c == 0, p, y), c, x)

    def second_peer(p):
        return (jnp.where(c == 0, p, z), jnp.where(c == 0, y, p), c, x)

    def other_core(device):
        return device[0], device[1], 1 - c, x

    barrier = pltpu.get_barrier_semaphore()
    peers = [x_peer(lax.rem(x + k, 4)) for k in (1, 2, 3)]
    peers += [first_peer(lax.rem(first + k, 8)) for k in range(1, 8)]
    peers += [second_peer(lax.rem(second + k, 8)) for k in range(1, 8)]
    peers += [partner]
    peers += [other_core(second_peer(lax.rem(second + k, 8))) for k in range(1, 8)]
    peers += [other_core(first_peer(lax.rem(first + k, 8))) for k in range(1, 8)]
    loads = [
        pltpu.make_async_copy(gate_hbm, gate_in, in_sem.at[0]),
        pltpu.make_async_copy(up_hbm, up_in, in_sem.at[1]),
        pltpu.make_async_copy(down_hbm, down_in, in_sem.at[2]),
        pltpu.make_async_copy(tokens_hbm, tok, in_sem.at[3]),
        pltpu.make_async_copy(gain_hbm, gain_in, in_sem.at[4]),
    ]
    for load in loads:
        load.start()
    for peer in peers:
        pl.semaphore_signal(barrier, inc=1, device_id=peer, device_id_type=MESH)

    lanes = lax.broadcasted_iota(jnp.int32, (32, 32), 1)
    rows = lax.broadcasted_iota(jnp.int32, (32, 32), 0)
    loads[4].wait()
    spread = jnp.broadcast_to(gain_in[...], (32, 32))
    gain = jnp.sum(jnp.where(lanes == rows, spread, 0.0), axis=1, keepdims=True)
    loads[0].wait()
    loads[1].wait()
    for s in range(4):
        scale = gain[8 * s : 8 * s + 8]
        g = gate_in[8 * s : 8 * s + 8, :] * scale
        u = up_in[8 * s : 8 * s + 8, :] * scale
        for j in range(16):
            cut = slice(176 * j, 176 * j + 176)
            unit = jnp.concatenate([g[:, cut], u[:, cut], jnp.zeros((8, 32), F32)], axis=1).astype(BF16)
            for n in range(3):
                packed[n, s, j // 8, j % 8] = unit[:, 128 * n : 128 * n + 128]

    pl.semaphore_wait(barrier, 32)
    x_sends = []
    for n in range(3):
        x_sends.append([])
        for k in (2, 1, 3):
            p = lax.rem(x + k, 4)
            x_sends[n].append(
                go(remote(packed.at[n, p], r1.at[n, pl.ds(2 * x, 2)], xs.at[n, k], xr.at[n, k], x_peer(p)))
            )

    loads[3].wait()

    def norm_rows(i, carry):
        part = tok[pl.ds(pl.multiple_of(16 * i, 16), 16), :].astype(F32)
        mean = jnp.mean(part * part, axis=-1, keepdims=True)
        normed[pl.ds(pl.multiple_of(16 * i, 16), 16), :] = (part * lax.rsqrt(mean + 1e-06)).astype(BF16)
        return carry

    lax.fori_loop(0, 12, norm_rows, 0)
    at = lax.broadcasted_iota(jnp.int32, (512, 256), 0)
    to = lax.broadcasted_iota(jnp.int32, (512, 256), 1)
    source = 64 * (to % 64 // 8) + 32 * c + 8 * (to // 64) + to % 8
    pick = jnp.where(at == source, 1.0, 0.0).astype(BF16)
    for q in range(4):
        even, odd = (
            jnp.dot(normed[:, 512 * v : 512 * v + 512], pick, preferred_element_type=F32).astype(BF16)
            for v in (2 * q, 2 * q + 1)
        )
        for s in range(4):
            cut = slice(64 * s, 64 * s + 64)
            tok_send[s, :, 128 * q : 128 * q + 128] = jnp.concatenate([even[:, cut], odd[:, cut]], axis=1)
    t_sends = []
    for k in (2, 1, 3):
        p = lax.rem(x + k, 4)
        t_sends.append(go(remote(tok_send.at[p], tok_all.at[x], ts.at[k], tr.at[k], x_peer(p))))
    tok_all[x] = tok_send[x]

    loads[2].wait()
    for i in range(11):
        db[c, x, i] = down_in[8 * i : 8 * i + 8, :].astype(BF16)

    def down_copy(t, h, k, p):
        half = db.at[c, t, :, :, pl.ds(512 * h, 512)]
        return remote(half, half, ds.at[k], dr.at[k], x_peer(p))

    d_ways = [
        go(down_copy(x, 0, 0, right)), go(down_copy(x, 1, 1, left)),
        go(down_copy(x, 1, 2, right)), go(down_copy(x, 0, 3, left)),
    ]

    def down_swap(t, k):
        return remote(db.at[c, t], db.at[c, t], es.at[k], er.at[k], partner)

    d_swaps = [go(down_swap(x, 0))]

    for n in range(3):
        r1[n, pl.ds(2 * x, 2)] = packed[n, x]

    a_sends = []
    for n in range(3):
        for send in x_sends[n]:
            land(send)
        a_sends.append([])
        for k in FAR_FIRST:
            p = lax.rem(first + k, 8)
            sems = as_.at[n, k], ar.at[n, k]

            @pl.when(c == 0)
            def _():
                remote(r1.at[n, :, p], r2.at[n, first], *sems, first_peer(p)).start()

            @pl.when(c == 1)
            def _():
                remote(r1.at[n, p], r2.at[n, first], *sems, first_peer(p)).start()

            a_sends[n].append(flights.note(remote(r1.at[n, p], r2.at[n, first], *sems, first_peer(p))))

        @pl.when(c == 0)
        def _():
            r2[n, first] = r1[n, :, first]

        @pl.when(c == 1)
        def _():
            r2[n, first] = r1[n, first]

    b_sends = []
    for n in range(3):
        for send in a_sends[n]:
            land(send)
        b_sends.append([])
        for k in FAR_FIRST:
            p = lax.rem(second + k, 8)
            sems = bs.at[n, k], br.at[n, k]

            @pl.when(c == 0)
            def _():
                remote(r2.at[n, :, p], w.at[n, second, :, c, x], *sems, second_peer(p)).start()

            @pl.when(c == 1)
            def _():
                remote(r2.at[n, :, p], w.at[n, :, second, c, x], *sems, second_peer(p)).start()

            b_sends[n].append(
                flights.note(remote(r2.at[n, :, p], w.at[n, second, :, c, x], *sems, second_peer(p)))
            )

        @pl.when(c == 0)
        def _():
            w[n, second, :, c, x] = r2[n, :, second]

        @pl.when(c == 1)
        def _():
            w[n, :, second, c, x] = r2[n, :, second]

    def gather_copy(s, n, h, k, p):
        half = w.at[n, :, pl.ds(4 * h, 4), c, s]
        return remote(half, half, gs.at[n, k], gr.at[n, k], x_peer(p))

    def core_copy(s, n, k):
        return remote(w.at[n, :, :, c, s], w.at[n, :, :, c, s], cs.at[n, k], cr.at[n, k], partner)

    for send in t_sends:
        land(send)
    u_sends = []
    for n in range(3):
        for send in b_sends[n]:
            land(send)
        part = jnp.dot(
            tok_all[...].reshape(768, 512), w[n, :, :, c, x].reshape(512, 128), preferred_element_type=F32
        ).reshape(4, 2, 96, 128)
        acc[n] = part

        @pl.when(c == 0)
        def _():
            core_send[n] = part[:, 1].astype(BF16)

        @pl.when(c == 1)
        def _():
            core_send[n] = part[:, 0].astype(BF16)

        u_sends.append(go(remote(core_send.at[n], core_got.at[n], us.at[n], ur.at[n], partner)))
        if n == 0:
            land(d_ways[0])
            d_ways.append(go(down_copy(left, 0, 4, right)))
            land(d_ways[1])
            d_ways.append(go(down_copy(right, 1, 5, left)))
            land(d_ways[2])
            d_swaps.append(go(down_swap(left, 1)))
            land(d_ways[3])
            d_swaps.append(go(down_swap(right, 2)))
    v_sends = []
    for n in range(3):
        land(u_sends[n])
        plane_send[n] = (acc[n, :, c] + core_got[n].astype(F32)).astype(BF16)
        v_sends.append([])
        for k in (2, 1, 3):
            p = lax.rem(x + k, 4)
            v_sends[n].append(
                go(remote(plane_send.at[n, p], plane_got.at[n, x], vs.at[n, k], vr.at[n, k], x_peer(p)))
            )
    for send in d_ways[4:]:
        land(send)
    d_swaps.append(go(down_swap(opposite, 3)))
    ways = []
    swaps = []
    for n in range(3):
        ways.append([
            go(gather_copy(x, n, 0, 0, right)), go(gather_copy(x, n, 1, 1, left)),
            go(gather_copy(x, n, 1, 2, right)), go(gather_copy(x, n, 0, 3, left)),
        ])
        swaps.append([go(core_copy(x, n, 0))])
    for send in d_swaps:
        land(send)

    @pl.when(c == 0)
    def _():
        for p in range(8):
            cols = [
                db[:, q // 2, :, :, 512 * (q % 2) + 64 * p : 512 * (q % 2) + 64 * p + 64].reshape(176, 64)
                for q in range(8)
            ]
            cols_of[p] = jnp.concatenate(cols, axis=1)

    @pl.when(c == 1)
    def _():
        for p in range(8):
            cols_of[p] = db[:, p // 2, :, :, 512 * (p % 2) : 512 * (p % 2) + 512].reshape(176, 512)

    sums = []
    for n in range(3):
        for send in v_sends[n]:
            land(send)
        total = acc[n, x, c] + core_got[n, x].astype(F32)
        for k in (1, 2, 3):
            total += plane_got[n, lax.rem(x + k, 4)].astype(F32)
        sums.append(total)
    gate = jnp.concatenate([sums[0], sums[1][:, :48]], axis=1)
    up = jnp.concatenate([sums[1][:, 48:], sums[2][:, :96]], axis=1)
    hidden = (gate * (1.0 / (1.0 + jnp.exp(-gate))) * up).astype(BF16)

    p_sends = []
    for k in (*FAR_FIRST, 0):
        p = lax.rem(first + k, 8)
        parts[p] = jnp.dot(hidden, cols_of[p], preferred_element_type=F32).astype(BF16)
        if k:
            p_sends.append(go(remote(parts.at[p], got.at[first], ps.at[k], pr.at[k], first_peer(p))))

    for t in range(4):
        down_out[:, :, 1024 * t : 1024 * t + 1024] = db[c, t]
    for n in range(3):
        land(ways[n][0])
        ways[n].append(go(gather_copy(left, n, 0, 4, right)))
        land(ways[n][1])
        ways[n].append(go(gather_copy(right, n, 1, 5, left)))
        land(ways[n][2])
        swaps[n].append(go(core_copy(left, n, 1)))
        land(ways[n][3])
        swaps[n].append(go(core_copy(right, n, 2)))

    q_sends = []
    total = parts[first].astype(F32)
    for k, send in zip(FAR_FIRST, p_sends):
        land(send)
        total += got[lax.rem(first + 8 - k, 8)].astype(F32)
    for q in range(16):
        groups = [total[32 * g : 32 * g + 32, 32 * q : 32 * q + 32] for g in range(3)]
        block = jnp.concatenate(groups + [jnp.zeros((32, 32), F32)], axis=1)
        pieces[q // 2, q % 2] = block.astype(BF16)
    for k in (*FAR_FIRST, 0):
        p = lax.rem(second + k, 8)
        for other in range(2):
            if k or other:
                d = 1 - c if other else c
                device = other_core(second_peer(p)) if other else second_peer(p)
                sems = qs.at[other, k], qr.at[other, k]
                q_sends.append(go(remote(pieces.at[p, d], got2.at[c, second], *sems, device)))
    got2[c, second] = pieces[second, c]
    for n in range(3):
        land(ways[n][4])
        land(ways[n][5])
        swaps[n].append(go(core_copy(opposite, n, 3)))
    for n in range(3):
        for send in swaps[n]:
            land(send)
        for core in range(2):
            @pl.when(c == core)
            def _():
                def unpack(i, carry):
                    at = pl.ds(pl.multiple_of(512 * i, 512), 512)
                    tile = w[n, i].reshape(512, 128).T
                    for out, start in ((gate_out, 88 * core), (up_out, 176 + 88 * core)):
                        for r in range(11):
                            k = start + 8 * r - 128 * n
                            if 0 <= k < 128:
                                out[r, :, at] = tile[k : k + 8]
                    return carry

                lax.fori_loop(0, 8, unpack, 0)
    for send in q_sends:
        land(send)
    blocks = []
    for core in range(2):
        total = got2[core, 0].astype(F32)
        for q in range(1, 8):
            total += got2[core, q].astype(F32)
        blocks += [total[:, 32 * g : 32 * g + 32] for g in range(3)]
    mixed_out[...] = jnp.concatenate(blocks, axis=0).T.astype(BF16)
    flights.finish()


def write_out(*refs):
    sem = refs[-1]
    copies = [pltpu.make_async_copy(refs[k], refs[k + 4], sem.at[k]) for k in range(4)]
    for copy in copies:
        copy.start()
    for copy in copies:
        copy.wait()


def on_device(prompt_tokens, norm_gain, gate_trained, up_trained, down_trained):
    dma = pltpu.SemaphoreType.DMA
    hbm = pl.BlockSpec(memory_space=pltpu.HBM)
    in_vmem = pl.BlockSpec(memory_space=pltpu.VMEM)
    vmem = pltpu.VMEM
    shapes = (
        jax.ShapeDtypeStruct((11, 8, 4096), BF16),
        jax.ShapeDtypeStruct((11, 8, 4096), BF16),
        jax.ShapeDtypeStruct((11, 8, 4096), BF16),
        jax.ShapeDtypeStruct((32, 192), BF16),
    )
    results = pl.pallas_call(
        kernel,
        out_shape=[pltpu.VMEM(a.shape, a.dtype) for a in shapes],
        in_specs=[hbm] * 5,
        out_specs=(in_vmem,) * 4,
        scratch_shapes=[
            vmem((192, 4096), BF16),
            vmem((1, 32), F32),
            vmem((32, 2816), F32),
            vmem((32, 2816), F32),
            vmem((88, 1024), F32),
            vmem((3, 4, 2, 8, 8, 128), BF16),
            vmem((3, 8, 8, 8, 128), BF16),
            vmem((3, 8, 8, 8, 128), BF16),
            vmem((3, 8, 8, 2, 4, 8, 128), BF16),
            vmem((192, 4096), BF16),
            vmem((4, 192, 512), BF16),
            vmem((4, 192, 512), BF16),
            vmem((3, 4, 2, 96, 128), F32),
            vmem((3, 4, 96, 128), BF16),
            vmem((3, 4, 96, 128), BF16),
            vmem((3, 4, 96, 128), BF16),
            vmem((3, 4, 96, 128), BF16),
            vmem((2, 4, 11, 8, 1024), BF16),
            vmem((8, 176, 512), BF16),
            vmem((8, 96, 512), BF16),
            vmem((8, 96, 512), BF16),
            vmem((8, 2, 32, 128), BF16),
            vmem((2, 8, 32, 128), BF16),
            dma((5,)),
            dma((4,)), dma((4,)),
            dma((3,)), dma((3,)),
            dma((3, 4)), dma((3, 4)),
            dma((3, 4)), dma((3, 4)),
            dma((3, 8)), dma((3, 8)),
            dma((3, 8)), dma((3, 8)),
            dma((6,)), dma((6,)),
            dma((3, 6)), dma((3, 6)),
            dma((3, 4)), dma((3, 4)),
            dma((4,)), dma((4,)),
            dma((8,)), dma((8,)),
            dma((2, 8)), dma((2, 8)),
        ],
        compiler_params=pltpu.CompilerParams(
            collective_id=0, has_side_effects=True, vmem_limit_bytes=LIMIT
        ),
    )(
        pltpu.with_memory_space_constraint(prompt_tokens, pltpu.HBM),
        pltpu.with_memory_space_constraint(norm_gain.reshape(1, 32), pltpu.HBM),
        pltpu.with_memory_space_constraint(gate_trained, pltpu.HBM),
        pltpu.with_memory_space_constraint(up_trained, pltpu.HBM),
        pltpu.with_memory_space_constraint(down_trained, pltpu.HBM),
    )
    gate, up, down, mixed = pl.pallas_call(
        write_out,
        out_shape=shapes,
        in_specs=[in_vmem] * 4,
        out_specs=(hbm,) * 4,
        scratch_shapes=[dma((4,))],
        compiler_params=pltpu.CompilerParams(vmem_limit_bytes=1024 * 1024),
    )(*results)
    return gate.reshape(88, 4096).T, up.reshape(88, 4096).T, down.reshape(88, 4096), mixed.T


def solution(mesh):
    finer = Mesh(mesh.devices.reshape(8, 8, 2, mesh.shape["tp"]), AXES)
    rows = AXES[:3]
    return jax.shard_map(
        on_device,
        mesh=finer,
        in_specs=(P("tp", None), P(rows), P(rows, "tp"), P(rows, "tp"), P(rows, "tp")),
        out_specs=(P(None, rows), P(None, rows), P(rows, None), P("tp", rows)),
        check_vma=False,
    )
```
